128 devices in a mesh: kv: 16 (over z, x), tp: 8 (over y, core).
Axes of the slice: x: 4, y: 4, z: 4, core: 2. Of those that a mesh axis runs over, the one named last changes fastest.
Arguments:
- tokens: bfloat16 [128, 4096], P('tp', 'kv'), may hold values from -16 to 16
- cache_keys: bfloat16 [128, 16384, 2, 128], P('tp', 'kv'), may hold values from -512 to 512
- cache_values: bfloat16 [128, 16384, 2, 128], P('tp', 'kv'), may hold values from -6 to 6
- attn_gain: float32 [4096], P('kv'), may hold values from 0.1 to 1.9
- w_query: bfloat16 [4096, 2048], P('kv'), may hold values from -0.15625 to 0.15625
- w_key: bfloat16 [4096, 256], P('kv'), may hold values from -0.09375 to 0.09375
- w_value: bfloat16 [4096, 256], P('kv'), may hold values from -0.09375 to 0.09375
- lambdas: float32 [16], replicated, may hold values from 0.3 to 0.8
- head_gain: float32 [128], replicated, may hold values from 0.1 to 1.9
- w_out: bfloat16 [2048, 4096], P(None, 'kv'), may hold values from -0.125 to 0.125
- mlp_gain: float32 [4096], P('kv'), may hold values from 0.1 to 1.9
- w_up: bfloat16 [4096, 16384], P('kv', 'tp'), may hold values from -0.09375 to 0.09375
- w_down: bfloat16 [16384, 4096], P('tp', 'kv'), may hold values from -0.046875 to 0.046875
Outputs:
- mixed: bfloat16 [128, 4096], P('tp', 'kv')
- new_keys: bfloat16 [128, 2, 128], P('tp')
- new_values: bfloat16 [128, 2, 128], P('tp')
The draws below stay inside these ranges and needn't reach their ends.
All inputs are finite; a program needn't handle non-finite values.
Results may differ from the reference program's by a relative error of at most 0.014.
Values may be sent and summed in bfloat16 or wider, within the bound.
A program may use at most 128 MiB of HBM per device.

```python
import jax
import jax.numpy as jnp
from jax import lax

D = 4096
HEADS = 16
KV_HEADS = 2
QK = 64
VD = 128
FF = 16384
BATCH = 128
CTX_DEV = 1024
CTX = 16384
N_KV = 16
N_TP = 8


def draw_tokens(key, part):
    key_scale, key_base = jax.random.split(jax.random.fold_in(key, 11))
    col_scales = jnp.exp(jax.random.uniform(key_scale, (D // 128,), jnp.float32, -1.2, 1.2))
    columns = jnp.repeat(col_scales, 128)
    base_vals = jax.random.normal(key_base, (BATCH, D), jnp.float32)
    return jnp.clip(base_vals * columns[None, :], -16.0, 16.0).astype(jnp.bfloat16)


def draw_cache_keys(key, part):
    key_base, key_mark = jax.random.split(jax.random.fold_in(key, 23))
    base_vals = jax.random.normal(key_base, (BATCH, CTX, KV_HEADS, 2 * QK), jnp.float32)
    return jnp.clip(base_vals, -512.0, 512.0).astype(jnp.bfloat16)


def steps_of(stream_key, shape, pieces, least, largest):
    factor_of = 1.0
    for position, blocks in pieces:
        heights = jax.random.uniform(jax.random.fold_in(jax.random.fold_in(stream_key, 6), position), (blocks,), jnp.float32, least / len(pieces), largest / len(pieces))
        factor_of = factor_of * jnp.repeat(jnp.exp(heights), shape[position] // blocks).reshape((-1,) + (1,) * (len(shape) - 1 - position))
    return factor_of


def normal_values(stream_key, extent, spread, bound, pieces=(), held_as=jnp.bfloat16):
    gain = steps_of(stream_key, extent, pieces, -0.22, 0.18) if pieces else 1.0
    values = jax.random.normal(stream_key, extent, jnp.float32) * spread * gain
    return jnp.minimum(jnp.maximum(values, -bound), bound).astype(held_as)


def setup_inputs(seed: int = 0) -> dict:
    splits = jax.random.split(jax.random.key(seed), 14)
    tokens = draw_tokens(jax.random.fold_in(splits[13], 71), 0)
    cache_keys = draw_cache_keys(jax.random.fold_in(splits[13], 71), 0)
    cache_values = normal_values(splits[2], (BATCH, CTX, KV_HEADS, VD), 1.0, 6.0, ((0, 8), (1, 16)))
    attn_gain = jnp.clip(1.0 + 0.18 * jax.random.normal(splits[3], (D,), jnp.float32), 0.1, 1.9)
    w_query = normal_values(splits[4], (D, HEADS * 2 * QK), (D // 3) ** -0.5, 0.15625, ((0, 16),))
    w_key = normal_values(splits[5], (D, KV_HEADS * 2 * QK), D ** -0.5, 0.09375, ((0, 16),))
    w_value = normal_values(splits[6], (D, KV_HEADS * VD), D ** -0.5, 0.09375, ((0, 16),))
    lambdas = jnp.clip(jax.random.uniform(splits[7], (HEADS,), jnp.float32, 0.3, 0.8), 0.3, 0.8)
    head_gain = jnp.clip(1.0 + 0.18 * jax.random.normal(splits[8], (VD,), jnp.float32), 0.1, 1.9)
    w_out = normal_values(splits[9], (HEADS * VD, D), (HEADS * VD) ** -0.5, 0.125, ((1, 16),))
    mlp_gain = jnp.clip(1.0 + 0.18 * jax.random.normal(splits[10], (D,), jnp.float32), 0.1, 1.9)
    w_up = normal_values(splits[11], (D, FF), D ** -0.5, 0.09375, ((0, 16), (1, 8)))
    w_down = normal_values(splits[12], (FF, D), FF ** -0.5, 0.046875, ((0, 8), (1, 16)))
    return dict(tokens=tokens, cache_keys=cache_keys, cache_values=cache_values, attn_gain=attn_gain, w_query=w_query, w_key=w_key, w_value=w_value, lambdas=lambdas, head_gain=head_gain, w_out=w_out, mlp_gain=mlp_gain, w_up=w_up, w_down=w_down)


norm_eps = 1e-06

def reference(tokens, cache_keys, cache_values, attn_gain, w_query, w_key, w_value, lambdas, head_gain, w_out, mlp_gain, w_up, w_down):
    tok_f = tokens.astype(jnp.float32)
    inv_one = lax.rsqrt(lax.optimization_barrier(jnp.mean(tok_f * tok_f, axis=1, keepdims=True)) + norm_eps)
    scaled = (tok_f * attn_gain[None, :]).astype(jnp.bfloat16)
    query = (jnp.dot(scaled, w_query, preferred_element_type=jnp.float32) * inv_one).astype(jnp.bfloat16)
    new_keys = (jnp.dot(scaled, w_key, preferred_element_type=jnp.float32) * inv_one).astype(jnp.bfloat16)
    new_values = (jnp.dot(scaled, w_value, preferred_element_type=jnp.float32) * inv_one).astype(jnp.bfloat16)
    head_group = HEADS // KV_HEADS
    query_five = query.reshape(BATCH, KV_HEADS, head_group, 2, QK).astype(jnp.float32)

    def one_block(index):
        begin = index * CTX_DEV
        keys_blk = lax.dynamic_slice_in_dim(cache_keys, begin, CTX_DEV, 1)
        keys_blk = keys_blk.reshape(BATCH, CTX_DEV, KV_HEADS, 2, QK).astype(jnp.float32)
        vals_blk = lax.dynamic_slice_in_dim(cache_values, begin, CTX_DEV, 1).astype(jnp.float32)
        scores = jnp.einsum('bkgcd,bpkcd->bkgcp', query_five, keys_blk) * QK ** (-0.5)
        block_top = lax.optimization_barrier(jnp.max(scores, axis=-1))
        exp_scores = jnp.exp(scores - block_top[..., None])
        block_total = lax.optimization_barrier(jnp.sum(exp_scores, axis=-1))
        weights = exp_scores.astype(jnp.bfloat16).astype(jnp.float32)
        block_acc = jnp.einsum('bkgcp,bpke->bkgce', weights, vals_blk)
        return (block_top, block_total, block_acc)
    tops, totals, accs = lax.map(one_block, jnp.arange(N_KV, dtype=jnp.int32))
    peak = lax.optimization_barrier(jnp.max(tops, axis=0))
    factor = jnp.exp(tops - peak[None])
    total = lax.optimization_barrier(jnp.sum(totals * factor, axis=0))
    acc = lax.optimization_barrier(jnp.sum(accs * factor[..., None], axis=0))
    lam_heads = lambdas.reshape(KV_HEADS, head_group)[None, :, :, None]
    head_out = acc[:, :, :, 0] / total[:, :, :, 0, None] - lam_heads * acc[:, :, :, 1] / total[:, :, :, 1, None]
    mean_sq = lax.optimization_barrier(jnp.mean(head_out * head_out, axis=-1, keepdims=True))
    normed = head_out * lax.rsqrt(mean_sq + 1.0 / CTX) * head_gain
    normed = normed.astype(jnp.bfloat16).reshape(BATCH, HEADS * VD)
    residual = (tok_f + jnp.dot(normed, w_out, preferred_element_type=jnp.float32)).astype(jnp.bfloat16)
    res_f = residual.astype(jnp.float32)
    inv_two = lax.rsqrt(lax.optimization_barrier(jnp.mean(res_f * res_f, axis=1, keepdims=True)) + norm_eps)
    gained = (res_f * mlp_gain[None, :]).astype(jnp.bfloat16)
    pre_act = jnp.dot(gained, w_up, preferred_element_type=jnp.float32) * inv_two
    act_rows = jnp.square(jax.nn.relu(pre_act)).astype(jnp.bfloat16)
    act_blocks = act_rows.reshape(BATCH, N_TP, FF // N_TP).astype(jnp.float32)
    down_blocks = w_down.reshape(N_TP, FF // N_TP, D).astype(jnp.float32)
    parts = jnp.einsum('btf,tfd->tbd', act_blocks, down_blocks)
    rounded = lax.optimization_barrier(parts.astype(jnp.bfloat16)).astype(jnp.float32)
    ffn_out = lax.optimization_barrier(jnp.sum(rounded, axis=0))
    mixed = (res_f + ffn_out).astype(jnp.bfloat16)
    return (mixed, new_keys.reshape(BATCH, KV_HEADS, 2 * QK), new_values.reshape(BATCH, KV_HEADS, VD))
```

```python
import functools

import jax
import jax.numpy as jnp
from jax import lax
from jax.experimental import pallas as pl
from jax.experimental.pallas import tpu as pltpu
from jax.sharding import PartitionSpec as P

norm_eps = 1e-06
f32 = jnp.float32
bf16 = jnp.bfloat16
VM = pl.BlockSpec(memory_space=pltpu.VMEM)
ANY = pl.BlockSpec(memory_space=pl.ANY)
DMA = pltpu.SemaphoreType.DMA
NT = (((1,), (1,)), ((), ()))
CHUNKS = 2
UNROLL = 2


def remote(src, dst, send, recv, axis, peer):
    return pltpu.make_async_remote_copy(
        src_ref=src,
        dst_ref=dst,
        send_sem=send,
        recv_sem=recv,
        device_id={axis: peer},
        device_id_type=pl.DeviceIdType.MESH,
    )


class Exchange:
    def __init__(self, axis, n, me, src_of, dst_of, send, recv):
        self.axis, self.n, self.me = axis, n, me
        self.src_of, self.dst_of, self.send, self.recv = src_of, dst_of, send, recv

    def copy(self, peer):
        me = self.me
        return remote(
            self.src_of(peer), self.dst_of(me), self.send.at[peer], self.recv.at[me], self.axis, peer
        )

    def start(self, k):
        self.copy(lax.rem(self.me + k, self.n)).start()

    def start_all(self):
        for k in range(1, self.n):
            self.start(k)

    def wait_from(self, peer):
        remote(
            self.src_of(peer), self.dst_of(peer), self.send.at[peer], self.recv.at[peer], self.axis, peer
        ).wait_recv()

    def wait_all(self):
        for k in range(1, self.n):
            self.wait_from(lax.rem(self.me + self.n - k, self.n))

    def drain(self):
        for k in range(1, self.n):
            self.copy(lax.rem(self.me + k, self.n)).wait_send()


def rows_of(start, size):
    return pl.ds(pl.multiple_of(start, size), size)


def layer_kernel(
    n,
    n_tp,
    kv_heads,
    full_width,
    ctx_total,
    scale,
    tokens,
    keys,
    values,
    attn_gain,
    w_query,
    w_key,
    w_value,
    lambdas,
    head_gain,
    w_out,
    mlp_gain,
    w_up,
    w_down,
    mixed,
    kv_out,
    tok_v,
    ag_v,
    wq_v,
    wk_v,
    wv_v,
    lam_v,
    hg_v,
    mg_v,
    kbuf,
    vbuf,
    wo_v,
    wu_v,
    wd_v,
    lsem,
    ksem,
    vsem,
    part_q,
    part_s,
    part_kv,
    got_q,
    got_s,
    got_kv,
    mine_q,
    mine_kv,
    all_q,
    acc,
    stat,
    gacc,
    gstat,
    mine_n,
    all_n,
    norm_f,
    res_v,
    all_res,
    sq_v,
    got_sq,
    up_v,
    got_up,
    mine_act,
    all_act,
    down_v,
    got_down,
    sems16,
    sems8,
    sems_up,
):
    me = lax.axis_index("kv")
    my_tp = lax.axis_index("tp")
    B = tokens.shape[0]
    heads = got_q.shape[1]
    half = heads // kv_heads
    lines = 2 * heads
    span = keys.shape[1]
    cols = tok_v.shape[1]
    all_rows = B * n_tp
    R = all_rows // CHUNKS
    groups = span // 128

    def ex(axis, i, src_of, dst_of):
        if axis == "kv":
            return Exchange("kv", n, me, src_of, dst_of, sems16.at[2 * i], sems16.at[2 * i + 1])
        return Exchange("tp", n_tp, my_tp, src_of, dst_of, sems8.at[2 * i], sems8.at[2 * i + 1])

    first = [(tokens, tok_v), (attn_gain, ag_v), (w_query, wq_v), (w_key, wk_v), (w_value, wv_v)]
    later = [
        (lambdas, lam_v),
        (head_gain, hg_v),
        (w_out, wo_v),
        (mlp_gain, mg_v),
        (w_up, wu_v),
        (w_down, wd_v),
    ]
    first = [pltpu.make_async_copy(a, b, lsem.at[i]) for i, (a, b) in enumerate(first)]
    later = [pltpu.make_async_copy(a, b, lsem.at[len(first) + i]) for i, (a, b) in enumerate(later)]
    for c in first:
        c.start()
    barrier = pltpu.get_barrier_semaphore()
    for axis, size, at in (("kv", n, me), ("tp", n_tp, my_tp)):
        for k in range(1, size):
            pl.semaphore_signal(
                barrier,
                inc=1,
                device_id={axis: lax.rem(at + k, size)},
                device_id_type=pl.DeviceIdType.MESH,
            )
    for c in first:
        c.wait()

    def fetch(b):
        return (
            pltpu.make_async_copy(keys.at[b], kbuf.at[b], ksem.at[b]),
            pltpu.make_async_copy(values.at[b], vbuf.at[b], vsem.at[b]),
        )

    def fetch_step(j, carry):
        for c in fetch(lax.rem(me + 1 + j, n)):
            c.start()
        return carry

    lax.fori_loop(0, B, fetch_step, 0)
    for c in later:
        c.start()

    tok_f = tok_v[...].astype(f32)
    scaled = (tok_f * ag_v[...]).astype(bf16)
    squares = jnp.broadcast_to(jnp.sum(tok_f * tok_f, axis=1, keepdims=True), (B, 128))
    for r in range(B):
        part_s[r] = squares[r : r + 1]
    product = jnp.dot(scaled, wq_v[...], preferred_element_type=f32)
    for h in range(heads):
        part_q[pl.ds(h, B, stride=heads), :] = product[:, h * 128 : (h + 1) * 128]
    pieces = 0
    for w in (wk_v, wv_v):
        product = jnp.dot(scaled, w[...], preferred_element_type=f32)
        for h in range(product.shape[1] // 128):
            part_kv[pl.ds(pieces, B, stride=8), :] = product[:, h * 128 : (h + 1) * 128]
            pieces += 1
    for h in range(pieces, 8):
        part_kv[pl.ds(h, B, stride=8), :] = jnp.zeros((B, 128), f32)

    x_q = ex("kv", 0, lambda p: part_q.at[rows_of(p * heads, heads)], lambda p: got_q.at[p])
    x_s = ex("kv", 1, lambda p: part_s.at[p], lambda p: got_s.at[p])
    x_kv = ex("kv", 2, lambda p: part_kv.at[rows_of(p * 8, 8)], lambda p: got_kv.at[p])
    pl.semaphore_wait(barrier, n - 1 + n_tp - 1)
    for k in range(1, n):
        x_s.start(k)
        x_q.start(k)
    x_kv.start_all()
    got_q[me] = part_q[rows_of(me * heads, heads), :]
    got_s[me] = part_s[me]
    got_kv[me] = part_kv[rows_of(me * 8, 8), :]
    x_s.wait_all()
    total = got_s[0]
    for k in range(1, n):
        total = total + got_s[k]
    inv_one = lax.rsqrt(total / full_width + norm_eps)
    x_q.wait_all()
    total = got_q[0]
    for k in range(1, n):
        total = total + got_q[k]
    query = (total * inv_one).astype(bf16).astype(f32) * scale
    mine_q[...] = query.astype(bf16)
    x_q2 = ex("kv", 3, lambda p: mine_q, lambda p: all_q.at[p])
    x_q2.start_all()
    all_q[me] = mine_q[...]
    x_kv.wait_all()
    total = got_kv[0]
    for k in range(1, n):
        total = total + got_kv[k]
    mine_kv[...] = (total * inv_one).astype(bf16)
    x_kv2 = ex("kv", 4, lambda p: mine_kv, lambda p: kv_out.at[p])
    x_kv2.start_all()
    kv_out[me] = mine_kv[...]

    lane = lax.broadcasted_iota(jnp.int32, (heads, 128), 1)
    even = lax.rem(lane, 2) == 0
    low = lane < 64
    diag = lax.broadcasted_iota(jnp.int32, (lines, 128), 1) == lax.broadcasted_iota(
        jnp.int32, (lines, 128), 0
    )

    x_acc = ex("kv", 5, lambda p: acc.at[p], lambda p: gacc.at[p])
    x_stat = ex("kv", 6, lambda p: stat.at[p], lambda p: gstat.at[p])

    def dest(j):
        return lax.rem(me + 1 + j, n)

    def one_row(b):
        q = all_q[b].astype(f32)
        lo = jnp.where(low, q, 0.0)
        hi = jnp.where(low, 0.0, q)
        q_lines = jnp.concatenate([lo[:half], hi[:half], lo[half:], hi[half:]], axis=0).astype(bf16)
        s = lax.dot_general(q_lines, kbuf[b], NT, preferred_element_type=f32)
        m = [
            jnp.where(even, s[:heads, c * 128 : (c + 1) * 128], s[heads:, c * 128 : (c + 1) * 128])
            for c in range(groups)
        ]
        top = m[0]
        for c in range(1, groups):
            top = jnp.maximum(top, m[c])
        top0 = jnp.max(jnp.where(even, top, -jnp.inf), axis=1, keepdims=True)
        top1 = jnp.max(jnp.where(even, -jnp.inf, top), axis=1, keepdims=True)
        top = jnp.where(even, top0, top1)
        m = [jnp.exp(x - top) for x in m]
        total = m[0]
        for c in range(1, groups):
            total = total + m[c]
        tot0 = jnp.sum(jnp.where(even, total, 0.0), axis=1, keepdims=True)
        tot1 = jnp.sum(jnp.where(even, 0.0, total), axis=1, keepdims=True)
        e = jnp.concatenate(
            [
                jnp.concatenate([jnp.where(even, x, 0.0).astype(bf16) for x in m], axis=1),
                jnp.concatenate([jnp.where(even, 0.0, x).astype(bf16) for x in m], axis=1),
            ],
            axis=0,
        )
        o = jnp.dot(e, vbuf[b], preferred_element_type=f32)
        tops = jnp.concatenate([top0, top1], axis=0)
        tots = jnp.concatenate([tot0, tot1], axis=0)
        row0 = jnp.sum(jnp.where(diag, tops, 0.0), axis=0, keepdims=True)
        row1 = jnp.sum(jnp.where(diag, tots, 0.0), axis=0, keepdims=True)
        return o.astype(bf16), jnp.concatenate([row0, row1], axis=0)

    def step(i, carry):
        bs = [dest(i * UNROLL + u) for u in range(UNROLL)]
        for u, b in enumerate(bs):
            if u == UNROLL - 1:

                @pl.when(b != me)
                def _(b=b):
                    x_q2.wait_from(b)

            else:
                x_q2.wait_from(b)
            for c in fetch(b):
                c.wait()
        results = [one_row(b) for b in bs]
        for u, (b, (o, st)) in enumerate(zip(bs, results)):
            acc[b] = o
            stat[b] = st
        for u, b in enumerate(bs):
            if u == UNROLL - 1:

                @pl.when(b != me)
                def _(b=b):
                    x_acc.copy(b).start()
                    x_stat.copy(b).start()

            else:
                x_acc.copy(b).start()
                x_stat.copy(b).start()
        return carry

    lax.fori_loop(0, B // UNROLL, step, 0)
    gacc[me] = acc[me]
    gstat[me] = stat[me]
    for c in later:
        c.wait()
    lam = jnp.broadcast_to(lam_v[...], (heads, heads))
    lam = jnp.sum(
        jnp.where(
            lax.broadcasted_iota(jnp.int32, (heads, heads), 0)
            == lax.broadcasted_iota(jnp.int32, (heads, heads), 1),
            lam,
            0.0,
        ),
        axis=1,
        keepdims=True,
    )
    x_stat.wait_all()
    tops = [gstat[k][0:1] for k in range(n)]
    peak = tops[0]
    for t in tops[1:]:
        peak = jnp.maximum(peak, t)
    facs = [jnp.exp(t - peak) for t in tops]
    total = facs[0] * gstat[0][1:2]
    for k in range(1, n):
        total = total + facs[k] * gstat[k][1:2]
    table = jnp.transpose(
        jnp.concatenate(facs + [jnp.broadcast_to(total, (8, 128))], axis=0)
    )
    x_acc.wait_all()
    merged = table[:lines, 0:1] * gacc[0].astype(f32)
    for k in range(1, n):
        merged = merged + table[:lines, k : k + 1] * gacc[k].astype(f32)
    ratio = merged / table[:lines, n : n + 1]
    normed = []
    for g in range(kv_heads):
        base = g * 2 * half
        head = ratio[base : base + half] - lam[g * half : (g + 1) * half] * ratio[base + half : base + 2 * half]
        mean_sq = jnp.mean(head * head, axis=1, keepdims=True)
        normed.append(head * lax.rsqrt(mean_sq + 1.0 / ctx_total) * hg_v[...])
    mine_n[...] = jnp.concatenate(normed, axis=0).astype(bf16)
    x_n = ex("kv", 7, lambda p: mine_n, lambda p: all_n.at[p])
    x_n.start_all()
    all_n[me] = mine_n[...]
    x_n.wait_all()

    for b in range(B):
        norm_f[b * heads : (b + 1) * heads, :] = all_n[b].astype(f32)
    normed = jnp.concatenate(
        [norm_f[pl.ds(h, B, stride=heads), :].astype(bf16) for h in range(heads)], axis=1
    )
    attn_out = jnp.dot(normed, wo_v[...], preferred_element_type=f32)
    res_v[...] = (tok_v[...].astype(f32) + attn_out).astype(bf16)
    x_res = ex("tp", 0, lambda p: res_v, lambda p: all_res.at[p])
    x_res.start_all()
    all_res[my_tp] = res_v[...]
    x_res.wait_all()

    every = all_res[...].reshape(all_rows, cols).astype(f32)
    gained = (every * mg_v[...]).astype(bf16)
    row_sq = jnp.sum(every * every, axis=1, keepdims=True)
    square = lax.broadcasted_iota(jnp.int32, (all_rows, all_rows), 0) == lax.broadcasted_iota(
        jnp.int32, (all_rows, all_rows), 1
    )
    sq_v[...] = jnp.sum(jnp.where(square, row_sq, 0.0), axis=0, keepdims=True)
    x_sq = ex("kv", 8, lambda p: sq_v, lambda p: got_sq.at[p])
    x_sq.start_all()
    got_sq[me] = sq_v[...]
    cw = up_v.shape[2]

    def chunk(ref, c):
        return ref.at[pl.ds(c * R, R)]

    x_up = [
        Exchange(
            "kv",
            n,
            me,
            lambda p, c=c: up_v.at[p, pl.ds(c * R, R)],
            lambda p, c=c: got_up.at[p, pl.ds(c * R, R)],
            sems_up.at[0, c],
            sems_up.at[1, c],
        )
        for c in range(CHUNKS)
    ]
    x_act = [
        Exchange(
            "kv",
            n,
            me,
            lambda p, c=c: mine_act.at[pl.ds(c * R, R)],
            lambda p, c=c: all_act.at[p, pl.ds(c * R, R)],
            sems_up.at[2, c],
            sems_up.at[3, c],
        )
        for c in range(CHUNKS)
    ]

    def up_of(peer):
        w = wu_v[:, rows_of(peer * cw, cw)]
        return jnp.dot(gained, w, preferred_element_type=f32).astype(bf16)

    def up_step(k, carry):
        peer = lax.rem(me + k, n)
        up_v[peer] = up_of(peer)
        x_up[0].copy(peer).start()
        return carry

    lax.fori_loop(1, n, up_step, 0)
    for c in range(1, CHUNKS):
        x_up[c].start_all()
    got_up[me] = up_of(me)
    x_sq.wait_all()
    total = got_sq[0]
    for k in range(1, n):
        total = total + got_sq[k]
    inv_row = lax.rsqrt(total / full_width + norm_eps)
    inv_two = jnp.sum(jnp.where(square, inv_row, 0.0), axis=1, keepdims=True)
    for c in range(CHUNKS):
        at = pl.ds(c * R, R)
        x_up[c].wait_all()
        total = got_up[0, at].astype(f32)
        for k in range(1, n):
            total = total + got_up[k, at].astype(f32)
        pre = jnp.maximum(total * inv_two[c * R : (c + 1) * R], 0.0)
        mine_act[at, :] = (pre * pre).astype(bf16)
        x_act[c].start_all()
        all_act[me, at] = mine_act[at, :]

    x_down = ex("tp", 1, lambda p: down_v.at[rows_of(p * B, B)], lambda p: got_down.at[p])
    for c in range(CHUNKS):
        at = pl.ds(c * R, R)
        x_act[c].wait_all()
        act = jnp.concatenate([all_act[k, at] for k in range(n)], axis=1)
        down_v[at, :] = jnp.dot(act, wd_v[...], preferred_element_type=f32).astype(bf16)
        for p in range(c * R // B, (c + 1) * R // B):

            @pl.when(my_tp != p)
            def _(p=p):
                x_down.copy(p).start()

    got_down[my_tp] = down_v[rows_of(my_tp * B, B), :]
    x_down.wait_all()
    total = got_down[0].astype(f32)
    for k in range(1, n_tp):
        total = total + got_down[k].astype(f32)
    mixed[...] = (res_v[...].astype(f32) + total).astype(bf16)

    x_kv2.wait_all()
    for x in [x_s, x_q, x_kv, x_q2, x_kv2, x_acc, x_stat, x_n, x_res, x_sq, x_down] + x_up + x_act:
        x.drain()


def shards(
    tokens,
    cache_keys,
    cache_values,
    attn_gain,
    w_query,
    w_key,
    w_value,
    lambdas,
    head_gain,
    w_out,
    mlp_gain,
    w_up,
    w_down,
):
    B, tok_width = tokens.shape
    n = lax.axis_size("kv")
    n_tp = lax.axis_size("tp")
    kv_heads = cache_keys.shape[2]
    comp = cache_keys.shape[3] // 2
    vd = cache_values.shape[3]
    ctx = cache_keys.shape[1]
    heads = lambdas.shape[0]
    span = ctx * kv_heads
    all_rows = B * n_tp
    hidden = w_up.shape[1]
    cw = hidden // n
    lines = 2 * heads
    assert B == n and comp * 2 == 128 and vd == 128
    V = pltpu.VMEM
    scratch = [
        V(tokens.shape, bf16),
        V((1, tok_width), f32),
        V(w_query.shape, bf16),
        V(w_key.shape, bf16),
        V(w_value.shape, bf16),
        V((1, heads), f32),
        V((1, vd), f32),
        V((1, tok_width), f32),
        V((B, span, 128), bf16),
        V((B, span, 128), bf16),
        V(w_out.shape, bf16),
        V(w_up.shape, bf16),
        V(w_down.shape, bf16),
        DMA((11,)),
        DMA((B,)),
        DMA((B,)),
        V((B * heads, 128), f32),
        V((B, 1, 128), f32),
        V((B * 8, 128), f32),
        V((n, heads, 128), f32),
        V((n, 1, 128), f32),
        V((n, 8, 128), f32),
        V((heads, 128), bf16),
        V((8, 128), bf16),
        V((n, heads, 128), bf16),
        V((n, lines, vd), bf16),
        V((n, 2, 128), f32),
        V((n, lines, vd), bf16),
        V((n, 2, 128), f32),
        V((heads, vd), bf16),
        V((n, heads, vd), bf16),
        V((B * heads, vd), f32),
        V((B, tok_width), bf16),
        V((n_tp, B, tok_width), bf16),
        V((1, all_rows), f32),
        V((n, 1, all_rows), f32),
        V((n, all_rows, cw), bf16),
        V((n, all_rows, cw), bf16),
        V((all_rows, cw), bf16),
        V((n, all_rows, cw), bf16),
        V((all_rows, tok_width), bf16),
        V((n_tp, B, tok_width), bf16),
        DMA((18, n)),
        DMA((4, n_tp)),
        DMA((4, CHUNKS, n)),
    ]
    mixed, kv_out = pl.pallas_call(
        functools.partial(
            layer_kernel, n, n_tp, kv_heads, tok_width * n, ctx * n, comp ** (-0.5)
        ),
        out_shape=(
            jax.ShapeDtypeStruct((B, tok_width), bf16),
            jax.ShapeDtypeStruct((n, 8, 128), bf16),
        ),
        in_specs=[ANY] * 13,
        out_specs=(VM, VM),
        scratch_shapes=scratch,
        compiler_params=pltpu.CompilerParams(
            collective_id=0, has_side_effects=True, vmem_limit_bytes=60 * 1024 * 1024
        ),
    )(
        tokens,
        cache_keys.reshape(B, span, 128),
        cache_values.reshape(B, span, vd),
        attn_gain.reshape(1, tok_width),
        w_query,
        w_key,
        w_value,
        lambdas.reshape(1, heads),
        head_gain.reshape(1, vd),
        w_out,
        mlp_gain.reshape(1, tok_width),
        w_up,
        w_down,
    )
    return mixed, kv_out[:, :kv_heads], kv_out[:, kv_heads : 2 * kv_heads]


def solution(mesh):
    in_specs = (
        P("tp", "kv"),
        P("tp", "kv", None, None),
        P("tp", "kv", None, None),
        P("kv"),
        P("kv", None),
        P("kv", None),
        P("kv", None),
        P(),
        P(),
        P(None, "kv"),
        P("kv"),
        P("kv", "tp"),
        P("tp", "kv"),
    )
    out_specs = (P("tp", "kv"), P("tp", None, None), P("tp", None, None))
    return jax.shard_map(shards, mesh=mesh, in_specs=in_specs, out_specs=out_specs, check_vma=False)
```

```python
import functools

import jax
import jax.numpy as jnp
from jax import lax
from jax.experimental import pallas as pl
from jax.experimental.pallas import tpu as pltpu
from jax.sharding import PartitionSpec as P

norm_eps = 1e-06
f32 = jnp.float32
bf16 = jnp.bfloat16
VM = pl.BlockSpec(memory_space=pltpu.VMEM)
HBM = pl.BlockSpec(memory_space=pltpu.HBM)
DMA = pltpu.SemaphoreType.DMA
NT = (((1,), (1,)), ((), ()))
CHUNKS = 2
UNROLL = 2


def remote(src, dst, send, recv, axis, peer):
    return pltpu.make_async_remote_copy(
        src_ref=src,
        dst_ref=dst,
        send_sem=send,
        recv_sem=recv,
        device_id={axis: peer},
        device_id_type=pl.DeviceIdType.MESH,
    )


class Exchange:
    def __init__(self, axis, n, me, src_of, dst_of, all_dst, sems):
        self.axis, self.n, self.me = axis, n, me
        self.src_of, self.dst_of, self.all_dst = src_of, dst_of, all_dst
        self.send, self.recv = sems.at[0], sems.at[1]

    def copy(self, peer):
        return remote(
            self.src_of(peer), self.dst_of(self.me), self.send, self.recv, self.axis, peer
        )

    def start(self, k):
        self.copy(lax.rem(self.me + k, self.n)).start()

    def start_all(self):
        for k in range(1, self.n):
            self.start(k)

    def everything(self):
        other = lax.rem(self.me + 1, self.n)
        return remote(self.all_dst, self.all_dst, self.send, self.recv, self.axis, other)

    def wait_all(self):
        self.everything().wait_recv()

    def drain(self):
        self.everything().wait_send()


def rows_of(start, size):
    return pl.ds(pl.multiple_of(start, size), size)


def layer_kernel(
    n,
    n_tp,
    kv_heads,
    full_width,
    ctx_total,
    scale,
    tokens,
    keys,
    values,
    attn_gain,
    w_query,
    w_key,
    w_value,
    lambdas,
    head_gain,
    w_out,
    mlp_gain,
    w_up,
    w_down,
    mixed,
    kv_out,
    tok_v,
    ag_v,
    wq_v,
    wk_v,
    wv_v,
    lam_v,
    hg_v,
    mg_v,
    kbuf,
    vbuf,
    wo_v,
    wu_v,
    wd_v,
    lsem,
    ksem,
    vsem,
    part_q,
    part_s,
    part_kv,
    got_q,
    got_s,
    got_kv,
    mine_q,
    mine_kv,
    all_q,
    acc,
    stat,
    gacc,
    gstat,
    mine_n,
    all_n,
    norm_f,
    res_v,
    all_res,
    sq_v,
    got_sq,
    up_v,
    got_up,
    mine_act,
    all_act,
    down_v,
    got_down,
    sems,
):
    me = lax.axis_index("kv")
    my_tp = lax.axis_index("tp")
    B = tokens.shape[0]
    heads = got_q.shape[1]
    half = heads // kv_heads
    lines = 2 * heads
    span = keys.shape[1]
    cols = tok_v.shape[1]
    all_rows = B * n_tp
    R = all_rows // CHUNKS
    groups = span // 128

    def ex(axis, i, src_of, dst):
        size, at = (n, me) if axis == "kv" else (n_tp, my_tp)
        return Exchange(
            axis, size, at, src_of, lambda p: dst.at[p], dst.at[pl.ds(0, size - 1)], sems.at[i]
        )

    first = [(tokens, tok_v), (attn_gain, ag_v), (w_query, wq_v), (w_key, wk_v), (w_value, wv_v)]
    later = [
        (lambdas, lam_v),
        (head_gain, hg_v),
        (w_out, wo_v),
        (mlp_gain, mg_v),
        (w_up, wu_v),
        (w_down, wd_v),
    ]
    first = [pltpu.make_async_copy(a, b, lsem.at[i]) for i, (a, b) in enumerate(first)]
    later = [pltpu.make_async_copy(a, b, lsem.at[len(first) + i]) for i, (a, b) in enumerate(later)]
    for c in first:
        c.start()
    barrier = pltpu.get_barrier_semaphore()
    for axis, size, at in (("kv", n, me), ("tp", n_tp, my_tp)):
        for k in range(1, size):
            pl.semaphore_signal(
                barrier,
                inc=1,
                device_id={axis: lax.rem(at + k, size)},
                device_id_type=pl.DeviceIdType.MESH,
            )
    for c in first:
        c.wait()

    def fetch(b):
        return (
            pltpu.make_async_copy(keys.at[b], kbuf.at[b], ksem),
            pltpu.make_async_copy(values.at[b], vbuf.at[b], vsem),
        )

    def fetch_step(j, carry):
        for c in fetch(lax.rem(me + 1 + j, n)):
            c.start()
        return carry

    lax.fori_loop(0, B, fetch_step, 0)
    for c in later:
        c.start()

    tok_f = tok_v[...].astype(f32)
    scaled = (tok_f * ag_v[...]).astype(bf16)
    squares = jnp.broadcast_to(jnp.sum(tok_f * tok_f, axis=1, keepdims=True), (B, 128))
    for r in range(B):
        part_s[r] = squares[r : r + 1]
    product = jnp.dot(scaled, wq_v[...], preferred_element_type=f32)
    for h in range(heads):
        part_q[pl.ds(h, B, stride=heads), :] = product[:, h * 128 : (h + 1) * 128]
    pieces = 0
    for w in (wk_v, wv_v):
        product = jnp.dot(scaled, w[...], preferred_element_type=f32)
        for h in range(product.shape[1] // 128):
            part_kv[pl.ds(pieces, B, stride=8), :] = product[:, h * 128 : (h + 1) * 128]
            pieces += 1
    for h in range(pieces, 8):
        part_kv[pl.ds(h, B, stride=8), :] = jnp.zeros((B, 128), f32)

    x_q = ex("kv", 0, lambda p: part_q.at[rows_of(p * heads, heads)], got_q)
    x_s = ex("kv", 1, lambda p: part_s.at[p], got_s)
    x_kv = ex("kv", 2, lambda p: part_kv.at[rows_of(p * 8, 8)], got_kv)
    pl.semaphore_wait(barrier, n - 1 + n_tp - 1)
    for k in range(1, n):
        x_s.start(k)
        x_q.start(k)
    x_kv.start_all()
    got_q[me] = part_q[rows_of(me * heads, heads), :]
    got_s[me] = part_s[me]
    got_kv[me] = part_kv[rows_of(me * 8, 8), :]
    x_s.wait_all()
    total = got_s[0]
    for k in range(1, n):
        total = total + got_s[k]
    inv_one = lax.rsqrt(total / full_width + norm_eps)
    x_q.wait_all()
    total = got_q[0]
    for k in range(1, n):
        total = total + got_q[k]
    query = (total * inv_one).astype(bf16).astype(f32) * scale
    mine_q[...] = query.astype(bf16)
    x_q2 = ex("kv", 3, lambda p: mine_q, all_q)
    x_q2.start_all()
    all_q[me] = mine_q[...]
    x_kv.wait_all()
    total = got_kv[0]
    for k in range(1, n):
        total = total + got_kv[k]
    new_kv = (total * inv_one).astype(bf16)
    for i in range(2):
        mine_kv[i] = new_kv[i * kv_heads : (i + 1) * kv_heads]
    x_kv2 = ex("kv", 4, lambda p: mine_kv, kv_out)
    x_kv2.start_all()
    kv_out[me] = mine_kv[...]

    lane = lax.broadcasted_iota(jnp.int32, (heads, 128), 1)
    even = lax.rem(lane, 2) == 0
    low = lane < 64
    diag = lax.broadcasted_iota(jnp.int32, (lines, 128), 1) == lax.broadcasted_iota(
        jnp.int32, (lines, 128), 0
    )

    x_acc = ex("kv", 5, lambda p: acc.at[p], gacc)
    x_stat = ex("kv", 6, lambda p: stat.at[p], gstat)

    def dest(j):
        return lax.rem(me + 1 + j, n)

    def one_row(b):
        q = all_q[b].astype(f32)
        lo = jnp.where(low, q, 0.0)
        hi = jnp.where(low, 0.0, q)
        q_lines = jnp.concatenate([lo[:half], hi[:half], lo[half:], hi[half:]], axis=0).astype(bf16)
        s = lax.dot_general(q_lines, kbuf[b], NT, preferred_element_type=f32)
        m = [
            jnp.where(even, s[:heads, c * 128 : (c + 1) * 128], s[heads:, c * 128 : (c + 1) * 128])
            for c in range(groups)
        ]
        top = m[0]
        for c in range(1, groups):
            top = jnp.maximum(top, m[c])
        top0 = jnp.max(jnp.where(even, top, -jnp.inf), axis=1, keepdims=True)
        top1 = jnp.max(jnp.where(even, -jnp.inf, top), axis=1, keepdims=True)
        top = jnp.where(even, top0, top1)
        m = [jnp.exp(x - top) for x in m]
        total = m[0]
        for c in range(1, groups):
            total = total + m[c]
        tot0 = jnp.sum(jnp.where(even, total, 0.0), axis=1, keepdims=True)
        tot1 = jnp.sum(jnp.where(even, 0.0, total), axis=1, keepdims=True)
        e = jnp.concatenate(
            [
                jnp.concatenate([jnp.where(even, x, 0.0).astype(bf16) for x in m], axis=1),
                jnp.concatenate([jnp.where(even, 0.0, x).astype(bf16) for x in m], axis=1),
            ],
            axis=0,
        )
        o = jnp.dot(e, vbuf[b], preferred_element_type=f32)
        tops = jnp.concatenate([top0, top1], axis=0)
        tots = jnp.concatenate([tot0, tot1], axis=0)
        row0 = jnp.sum(jnp.where(diag, tops, 0.0), axis=0, keepdims=True)
        row1 = jnp.sum(jnp.where(diag, tots, 0.0), axis=0, keepdims=True)
        return o.astype(bf16), jnp.concatenate([row0, row1], axis=0)

    def step(i, carry):
        bs = [dest(i * UNROLL + u) for u in range(UNROLL)]
        results = [one_row(b) for b in bs]
        for u, (b, (o, st)) in enumerate(zip(bs, results)):
            acc[b] = o
            stat[b] = st
        for u, b in enumerate(bs):
            if u == UNROLL - 1:

                @pl.when(b != me)
                def _(b=b):
                    x_acc.copy(b).start()
                    x_stat.copy(b).start()

            else:
                x_acc.copy(b).start()
                x_stat.copy(b).start()
        return carry

    x_q2.wait_all()
    pltpu.make_async_copy(keys, kbuf, ksem).wait()
    pltpu.make_async_copy(values, vbuf, vsem).wait()
    lax.fori_loop(0, B // UNROLL, step, 0)
    gacc[me] = acc[me]
    gstat[me] = stat[me]
    for c in later:
        c.wait()
    lam = jnp.broadcast_to(lam_v[...], (heads, heads))
    lam = jnp.sum(
        jnp.where(
            lax.broadcasted_iota(jnp.int32, (heads, heads), 0)
            == lax.broadcasted_iota(jnp.int32, (heads, heads), 1),
            lam,
            0.0,
        ),
        axis=1,
        keepdims=True,
    )
    x_stat.wait_all()
    tops = [gstat[k][0:1] for k in range(n)]
    peak = tops[0]
    for t in tops[1:]:
        peak = jnp.maximum(peak, t)
    facs = [jnp.exp(t - peak) for t in tops]
    total = facs[0] * gstat[0][1:2]
    for k in range(1, n):
        total = total + facs[k] * gstat[k][1:2]
    table = jnp.transpose(
        jnp.concatenate(facs + [jnp.broadcast_to(total, (8, 128))], axis=0)
    )
    x_acc.wait_all()
    merged = table[:lines, 0:1] * gacc[0].astype(f32)
    for k in range(1, n):
        merged = merged + table[:lines, k : k + 1] * gacc[k].astype(f32)
    ratio = merged / table[:lines, n : n + 1]
    normed = []
    for g in range(kv_heads):
        base = g * 2 * half
        head = ratio[base : base + half] - lam[g * half : (g + 1) * half] * ratio[base + half : base + 2 * half]
        mean_sq = jnp.mean(head * head, axis=1, keepdims=True)
        normed.append(head * lax.rsqrt(mean_sq + 1.0 / ctx_total) * hg_v[...])
    mine_n[...] = jnp.concatenate(normed, axis=0).astype(bf16)
    x_n = ex("kv", 7, lambda p: mine_n, all_n)
    x_n.start_all()
    all_n[me] = mine_n[...]
    x_n.wait_all()

    for b in range(B):
        norm_f[b * heads : (b + 1) * heads, :] = all_n[b].astype(f32)
    normed = jnp.concatenate(
        [norm_f[pl.ds(h, B, stride=heads), :].astype(bf16) for h in range(heads)], axis=1
    )
    attn_out = jnp.dot(normed, wo_v[...], preferred_element_type=f32)
    res_v[...] = (tok_v[...].astype(f32) + attn_out).astype(bf16)
    x_res = ex("tp", 9, lambda p: res_v, all_res)
    x_res.start_all()
    all_res[my_tp] = res_v[...]
    x_res.wait_all()

    every = all_res[...].reshape(all_rows, cols).astype(f32)
    gained = (every * mg_v[...]).astype(bf16)
    row_sq = jnp.sum(every * every, axis=1, keepdims=True)
    square = lax.broadcasted_iota(jnp.int32, (all_rows, all_rows), 0) == lax.broadcasted_iota(
        jnp.int32, (all_rows, all_rows), 1
    )
    sq_v[...] = jnp.sum(jnp.where(square, row_sq, 0.0), axis=0, keepdims=True)
    x_sq = ex("kv", 8, lambda p: sq_v, got_sq)
    x_sq.start_all()
    got_sq[me] = sq_v[...]
    cw = up_v.shape[2]

    x_up, x_act = [], []
    for c in range(CHUNKS):
        at = pl.ds(c * R, R)
        for xs, src_of, dst, i in (
            (x_up, lambda p, at=at: up_v.at[p, at], got_up, 11 + 2 * c),
            (x_act, lambda p, at=at: mine_act.at[at], all_act, 12 + 2 * c),
        ):
            xs.append(
                Exchange(
                    "kv",
                    n,
                    me,
                    src_of,
                    lambda p, dst=dst, at=at: dst.at[p, at],
                    dst.at[pl.ds(0, n - 1), at],
                    sems.at[i],
                )
            )

    def up_of(peer):
        w = wu_v[:, rows_of(peer * cw, cw)]
        return jnp.dot(gained, w, preferred_element_type=f32).astype(bf16)

    def up_step(k, carry):
        peer = lax.rem(me + k, n)
        up_v[peer] = up_of(peer)
        x_up[0].copy(peer).start()
        return carry

    lax.fori_loop(1, n, up_step, 0)
    for c in range(1, CHUNKS):
        x_up[c].start_all()
    got_up[me] = up_of(me)
    x_sq.wait_all()
    total = got_sq[0]
    for k in range(1, n):
        total = total + got_sq[k]
    inv_row = lax.rsqrt(total / full_width + norm_eps)
    inv_two = jnp.sum(jnp.where(square, inv_row, 0.0), axis=1, keepdims=True)
    for c in range(CHUNKS):
        at = pl.ds(c * R, R)
        x_up[c].wait_all()
        total = got_up[0, at].astype(f32)
        for k in range(1, n):
            total = total + got_up[k, at].astype(f32)
        pre = jnp.maximum(total * inv_two[c * R : (c + 1) * R], 0.0)
        mine_act[at, :] = (pre * pre).astype(bf16)
        x_act[c].start_all()
        all_act[me, at] = mine_act[at, :]

    x_down = ex("tp", 10, lambda p: down_v.at[rows_of(p * B, B)], got_down)
    for c in range(CHUNKS):
        at = pl.ds(c * R, R)
        x_act[c].wait_all()
        act = jnp.concatenate([all_act[k, at] for k in range(n)], axis=1)
        down_v[at, :] = jnp.dot(act, wd_v[...], preferred_element_type=f32).astype(bf16)
        for p in range(c * R // B, (c + 1) * R // B):

            @pl.when(my_tp != p)
            def _(p=p):
                x_down.copy(p).start()

    got_down[my_tp] = down_v[rows_of(my_tp * B, B), :]
    x_down.wait_all()
    total = got_down[0].astype(f32)
    for k in range(1, n_tp):
        total = total + got_down[k].astype(f32)
    mixed[...] = (res_v[...].astype(f32) + total).astype(bf16)

    x_kv2.wait_all()
    for x in [x_s, x_q, x_kv, x_q2, x_kv2, x_acc, x_stat, x_n, x_res, x_sq, x_down] + x_up + x_act:
        x.drain()


def result_kernel(mixed, kv_out, out, new_keys, new_values, sems):
    copies = [
        pltpu.make_async_copy(src, dst, sems.at[i])
        for i, (src, dst) in enumerate(
            ((mixed, out), (kv_out.at[:, 0], new_keys), (kv_out.at[:, 1], new_values))
        )
    ]
    for c in copies:
        c.start()
    for c in copies:
        c.wait()


def shards(
    tokens,
    cache_keys,
    cache_values,
    attn_gain,
    w_query,
    w_key,
    w_value,
    lambdas,
    head_gain,
    w_out,
    mlp_gain,
    w_up,
    w_down,
):
    B, tok_width = tokens.shape
    n = lax.axis_size("kv")
    n_tp = lax.axis_size("tp")
    kv_heads = cache_keys.shape[2]
    comp = cache_keys.shape[3] // 2
    vd = cache_values.shape[3]
    ctx = cache_keys.shape[1]
    heads = lambdas.shape[0]
    span = ctx * kv_heads
    all_rows = B * n_tp
    hidden = w_up.shape[1]
    cw = hidden // n
    lines = 2 * heads
    assert B == n and comp * 2 == 128 and vd == 128
    V = pltpu.VMEM
    scratch = [
        V(tokens.shape, bf16),
        V((1, tok_width), f32),
        V(w_query.shape, bf16),
        V(w_key.shape, bf16),
        V(w_value.shape, bf16),
        V((1, heads), f32),
        V((1, vd), f32),
        V((1, tok_width), f32),
        V((B, span, 128), bf16),
        V((B, span, 128), bf16),
        V(w_out.shape, bf16),
        V(w_up.shape, bf16),
        V(w_down.shape, bf16),
        DMA((11,)),
        DMA,
        DMA,
        V((B * heads, 128), f32),
        V((B, 1, 128), f32),
        V((B * 8, 128), f32),
        V((n, heads, 128), f32),
        V((n, 1, 128), f32),
        V((n, 8, 128), f32),
        V((heads, 128), bf16),
        V((2, kv_heads, 128), bf16),
        V((n, heads, 128), bf16),
        V((n, lines, vd), bf16),
        V((n, 2, 128), f32),
        V((n, lines, vd), bf16),
        V((n, 2, 128), f32),
        V((heads, vd), bf16),
        V((n, heads, vd), bf16),
        V((B * heads, vd), f32),
        V((B, tok_width), bf16),
        V((n_tp, B, tok_width), bf16),
        V((1, all_rows), f32),
        V((n, 1, all_rows), f32),
        V((n, all_rows, cw), bf16),
        V((n, all_rows, cw), bf16),
        V((all_rows, cw), bf16),
        V((n, all_rows, cw), bf16),
        V((all_rows, tok_width), bf16),
        V((n_tp, B, tok_width), bf16),
        DMA((11 + 2 * CHUNKS, 2)),
    ]
    mixed, kv_out = pl.pallas_call(
        functools.partial(
            layer_kernel, n, n_tp, kv_heads, tok_width * n, ctx * n, comp ** (-0.5)
        ),
        out_shape=(
            jax.ShapeDtypeStruct((B, tok_width), bf16),
            jax.ShapeDtypeStruct((n, 2, kv_heads, 128), bf16),
        ),
        in_specs=[HBM] * 13,
        out_specs=(VM, VM),
        scratch_shapes=scratch,
        compiler_params=pltpu.CompilerParams(
            collective_id=0, has_side_effects=True, vmem_limit_bytes=48 * 1024 * 1024
        ),
    )(
        *[
            pltpu.with_memory_space_constraint(x, pltpu.HBM)
            for x in (
                tokens,
                cache_keys.reshape(B, span, 128),
                cache_values.reshape(B, span, vd),
                attn_gain.reshape(1, tok_width),
                w_query,
                w_key,
                w_value,
                lambdas.reshape(1, heads),
                head_gain.reshape(1, vd),
                w_out,
                mlp_gain.reshape(1, tok_width),
                w_up,
                w_down,
            )
        ]
    )
    return pl.pallas_call(
        result_kernel,
        out_shape=(
            jax.ShapeDtypeStruct(mixed.shape, bf16),
            jax.ShapeDtypeStruct((n, kv_heads, 128), bf16),
            jax.ShapeDtypeStruct((n, kv_heads, 128), bf16),
        ),
        in_specs=[VM, VM],
        out_specs=(HBM, HBM, HBM),
        scratch_shapes=[DMA((3,))],
        compiler_params=pltpu.CompilerParams(vmem_limit_bytes=1024 * 1024),
    )(mixed, kv_out)


def solution(mesh):
    in_specs = (
        P("tp", "kv"),
        P("tp", "kv", None, None),
        P("tp", "kv", None, None),
        P("kv"),
        P("kv", None),
        P("kv", None),
        P("kv", None),
        P(),
        P(),
        P(None, "kv"),
        P("kv"),
        P("kv", "tp"),
        P("tp", "kv"),
    )
    out_specs = (P("tp", "kv"), P("tp", None, None), P("tp", None, None))
    return jax.shard_map(shards, mesh=mesh, in_specs=in_specs, out_specs=out_specs, check_vma=False)
```

```python
import functools

import jax
import jax.numpy as jnp
from jax import lax
from jax.experimental import pallas as pl
from jax.experimental.pallas import tpu as pltpu
from jax.sharding import PartitionSpec as P

norm_eps = 1e-06
f32 = jnp.float32
bf16 = jnp.bfloat16
VM = pl.BlockSpec(memory_space=pltpu.VMEM)
HBM = pl.BlockSpec(memory_space=pltpu.HBM)
DMA = pltpu.SemaphoreType.DMA
NT = (((1,), (1,)), ((), ()))
UNROLL = 4


def remote(src, dst, send, recv, axis, peer):
    return pltpu.make_async_remote_copy(
        src_ref=src,
        dst_ref=dst,
        send_sem=send,
        recv_sem=recv,
        device_id={axis: peer},
        device_id_type=pl.DeviceIdType.MESH,
    )


class Exchange:
    def __init__(self, axis, peers, me, src_of, dst_of, all_dst, sems):
        self.axis, self.peers, self.me = axis, peers, me
        self.src_of, self.dst_of, self.all_dst = src_of, dst_of, all_dst
        self.send, self.recv = sems.at[0], sems.at[1]

    def copy(self, peer):
        return remote(
            self.src_of(peer), self.dst_of(self.me), self.send, self.recv, self.axis, peer
        )

    def start_all(self):
        for peer in self.peers:
            self.copy(peer).start()

    def everything(self):
        return remote(self.all_dst, self.all_dst, self.send, self.recv, self.axis, self.peers[0])

    def wait_all(self):
        self.everything().wait_recv()

    def drain(self):
        self.everything().wait_send()


def offsets(outer, inner, wrap_inner):
    def far(d, size, wrap):
        return min(d, size - d) if wrap else d % 2

    every = [(a, b) for a in range(outer) for b in range(inner)]
    every.sort(key=lambda o: -(far(o[0], outer, True) + far(o[1], inner, wrap_inner) / 1.5))
    return every


def rows_of(start, size):
    return pl.ds(pl.multiple_of(start, size), size)


def layer_kernel(
    n,
    n_tp,
    kv_heads,
    full_width,
    ctx_total,
    scale,
    tokens,
    keys,
    values,
    attn_gain,
    w_query,
    w_key,
    w_value,
    lambdas,
    head_gain,
    w_out,
    mlp_gain,
    w_up,
    w_down,
    mixed,
    kv_out,
    tok_v,
    ag_v,
    wq_v,
    wk_v,
    wv_v,
    lam_v,
    hg_v,
    mg_v,
    kbuf,
    vbuf,
    wo_v,
    wu_v,
    wd_v,
    lsem,
    ksem,
    vsem,
    part_q,
    part_s,
    part_kv,
    got_q,
    got_s,
    got_kv,
    mine_q,
    mine_kv,
    all_q,
    acc,
    stat,
    gacc,
    gstat,
    mine_n,
    all_n,
    norm_f,
    res_v,
    all_res,
    sq_v,
    got_sq,
    up_v,
    got_up,
    mine_act,
    all_act,
    down_v,
    got_down,
    sems,
    res_sem,
):
    me = lax.axis_index("kv")
    my_tp = lax.axis_index("tp")
    B = tokens.shape[0]
    heads = got_q.shape[1]
    half = heads // kv_heads
    lines = 2 * heads
    span = keys.shape[1]
    cols = tok_v.shape[1]
    all_rows = B * n_tp
    R = 2 * B
    groups = span // 128

    def order(at, outer, inner, wrap_inner):
        a, b = at // inner, lax.rem(at, inner)
        return [
            lax.rem(a + da, outer) * inner + lax.rem(b + db, inner)
            for da, db in offsets(outer, inner, wrap_inner)
        ]

    side = int(n**0.5)
    ny = n_tp // 2
    kv_order = order(me, side, side, True)
    kv_peers = kv_order[:-1]
    near_peers, far_peers = kv_order[-5:-1], kv_order[:-5]
    tp_peers = order(my_tp, ny, 2, False)[:-1]

    def ex(axis, i, src_of, dst, peers=None):
        every, at = (kv_peers, me) if axis == "kv" else (tp_peers, my_tp)
        peers = every if peers is None else peers
        return Exchange(
            axis, peers, at, src_of, lambda p: dst.at[p], dst.at[pl.ds(0, len(peers))], sems.at[i]
        )

    first = [(tokens, tok_v), (attn_gain, ag_v), (w_query, wq_v), (w_key, wk_v), (w_value, wv_v)]
    later = [
        (lambdas, lam_v),
        (head_gain, hg_v),
        (w_out, wo_v),
        (mlp_gain, mg_v),
        (w_up, wu_v),
        (w_down, wd_v),
    ]
    first = [pltpu.make_async_copy(a, b, lsem.at[i]) for i, (a, b) in enumerate(first)]
    later = [pltpu.make_async_copy(a, b, lsem.at[len(first) + i]) for i, (a, b) in enumerate(later)]
    for c in first:
        c.start()
    barrier = pltpu.get_barrier_semaphore()
    for axis, peers in (("kv", kv_peers), ("tp", tp_peers)):
        for peer in peers:
            pl.semaphore_signal(
                barrier, inc=1, device_id={axis: peer}, device_id_type=pl.DeviceIdType.MESH
            )
    for c in first:
        c.wait()

    def fetch(b):
        return (
            pltpu.make_async_copy(keys.at[b], kbuf.at[b], ksem),
            pltpu.make_async_copy(values.at[b], vbuf.at[b], vsem),
        )

    for b in kv_order:
        for c in fetch(b):
            c.start()
    for c in later:
        c.start()

    tok_f = tok_v[...].astype(f32)
    scaled = (tok_f * ag_v[...]).astype(bf16)
    squares = jnp.broadcast_to(jnp.sum(tok_f * tok_f, axis=1, keepdims=True), (B, 128))
    for r in range(B):
        part_s[r] = squares[r : r + 1]
    product = jnp.dot(scaled, wq_v[...], preferred_element_type=f32)
    for h in range(heads):
        part_q[pl.ds(h, B, stride=heads), :] = product[:, h * 128 : (h + 1) * 128]
    pieces = 0
    for w in (wk_v, wv_v):
        product = jnp.dot(scaled, w[...], preferred_element_type=f32)
        for h in range(product.shape[1] // 128):
            part_kv[pl.ds(pieces, B, stride=8), :] = product[:, h * 128 : (h + 1) * 128]
            pieces += 1
    for h in range(pieces, 8):
        part_kv[pl.ds(h, B, stride=8), :] = jnp.zeros((B, 128), f32)

    x_q = ex("kv", 0, lambda p: part_q.at[rows_of(p * heads, heads)], got_q)
    x_s = ex("kv", 1, lambda p: part_s.at[p], got_s)
    x_kv = ex("kv", 2, lambda p: part_kv.at[rows_of(p * 8, 8)], got_kv)
    pl.semaphore_wait(barrier, n - 1 + n_tp - 1)
    for peer in kv_peers:
        x_s.copy(peer).start()
        x_q.copy(peer).start()
    x_kv.start_all()
    got_q[me] = part_q[rows_of(me * heads, heads), :]
    got_s[me] = part_s[me]
    got_kv[me] = part_kv[rows_of(me * 8, 8), :]
    x_s.wait_all()
    total = got_s[0]
    for k in range(1, n):
        total = total + got_s[k]
    inv_one = lax.rsqrt(total / full_width + norm_eps)
    x_q.wait_all()
    total = got_q[0]
    for k in range(1, n):
        total = total + got_q[k]
    query = (total * inv_one).astype(bf16).astype(f32) * scale
    mine_q[...] = query.astype(bf16)
    x_far = ex("kv", 3, lambda p: mine_q, all_q, far_peers)
    x_near = ex("kv", 8, lambda p: mine_q, all_q, near_peers)
    x_far.start_all()
    x_near.start_all()
    all_q[me] = mine_q[...]
    x_kv.wait_all()
    total = got_kv[0]
    for k in range(1, n):
        total = total + got_kv[k]
    new_kv = (total * inv_one).astype(bf16)
    for i in range(2):
        mine_kv[i] = new_kv[i * kv_heads : (i + 1) * kv_heads]
    x_kv2 = ex("kv", 4, lambda p: mine_kv, kv_out)
    x_kv2.start_all()
    kv_out[me] = mine_kv[...]

    lane = lax.broadcasted_iota(jnp.int32, (heads, 128), 1)
    even = lax.rem(lane, 2) == 0
    low = lane < 64
    diag = lax.broadcasted_iota(jnp.int32, (lines, 128), 1) == lax.broadcasted_iota(
        jnp.int32, (lines, 128), 0
    )

    x_acc = ex("kv", 5, lambda p: acc.at[p], gacc)
    x_stat = ex("kv", 6, lambda p: stat.at[p], gstat)

    def one_row(b):
        q = all_q[b].astype(f32)
        lo = jnp.where(low, q, 0.0)
        hi = jnp.where(low, 0.0, q)
        q_lines = jnp.concatenate([lo[:half], hi[:half], lo[half:], hi[half:]], axis=0).astype(bf16)
        s = lax.dot_general(q_lines, kbuf[b], NT, preferred_element_type=f32)
        m = [
            jnp.where(even, s[:heads, c * 128 : (c + 1) * 128], s[heads:, c * 128 : (c + 1) * 128])
            for c in range(groups)
        ]
        top = m[0]
        for c in range(1, groups):
            top = jnp.maximum(top, m[c])
        top0 = jnp.max(jnp.where(even, top, -jnp.inf), axis=1, keepdims=True)
        top1 = jnp.max(jnp.where(even, -jnp.inf, top), axis=1, keepdims=True)
        top = jnp.where(even, top0, top1)
        m = [jnp.exp(x - top) for x in m]
        total = m[0]
        for c in range(1, groups):
            total = total + m[c]
        tot0 = jnp.sum(jnp.where(even, total, 0.0), axis=1, keepdims=True)
        tot1 = jnp.sum(jnp.where(even, 0.0, total), axis=1, keepdims=True)
        e = jnp.concatenate(
            [
                jnp.concatenate([jnp.where(even, x, 0.0).astype(bf16) for x in m], axis=1),
                jnp.concatenate([jnp.where(even, 0.0, x).astype(bf16) for x in m], axis=1),
            ],
            axis=0,
        )
        o = jnp.dot(e, vbuf[b], preferred_element_type=f32)
        tops = jnp.concatenate([top0, top1], axis=0)
        tots = jnp.concatenate([tot0, tot1], axis=0)
        row0 = jnp.sum(jnp.where(diag, tops, 0.0), axis=0, keepdims=True)
        row1 = jnp.sum(jnp.where(diag, tots, 0.0), axis=0, keepdims=True)
        return o.astype(bf16), jnp.concatenate([row0, row1], axis=0)

    def attend(bs, send=True):
        for b, (o, st) in zip(bs, [one_row(b) for b in bs]):
            acc[b] = o
            stat[b] = st
        for b in bs if send else ():
            x_acc.copy(b).start()
            x_stat.copy(b).start()

    pltpu.make_async_copy(keys, kbuf, ksem).wait()
    pltpu.make_async_copy(values, vbuf, vsem).wait()
    attend([me], send=False)
    x_near.wait_all()
    attend(near_peers)
    x_far.wait_all()
    for i in range(0, len(far_peers), UNROLL):
        attend(far_peers[i : i + UNROLL])
    gacc[me] = acc[me]
    gstat[me] = stat[me]
    for c in later:
        c.wait()
    lam = jnp.broadcast_to(lam_v[...], (heads, heads))
    lam = jnp.sum(
        jnp.where(
            lax.broadcasted_iota(jnp.int32, (heads, heads), 0)
            == lax.broadcasted_iota(jnp.int32, (heads, heads), 1),
            lam,
            0.0,
        ),
        axis=1,
        keepdims=True,
    )
    x_stat.wait_all()
    tops = [gstat[k][0:1] for k in range(n)]
    peak = tops[0]
    for t in tops[1:]:
        peak = jnp.maximum(peak, t)
    facs = [jnp.exp(t - peak) for t in tops]
    total = facs[0] * gstat[0][1:2]
    for k in range(1, n):
        total = total + facs[k] * gstat[k][1:2]
    table = jnp.transpose(
        jnp.concatenate(facs + [jnp.broadcast_to(total, (8, 128))], axis=0)
    )
    x_acc.wait_all()
    merged = table[:lines, 0:1] * gacc[0].astype(f32)
    for k in range(1, n):
        merged = merged + table[:lines, k : k + 1] * gacc[k].astype(f32)
    ratio = merged / table[:lines, n : n + 1]
    normed = []
    for g in range(kv_heads):
        base = g * 2 * half
        head = ratio[base : base + half] - lam[g * half : (g + 1) * half] * ratio[base + half : base + 2 * half]
        mean_sq = jnp.mean(head * head, axis=1, keepdims=True)
        normed.append(head * lax.rsqrt(mean_sq + 1.0 / ctx_total) * hg_v[...])
    mine_n[...] = jnp.concatenate(normed, axis=0).astype(bf16)
    x_n = ex("kv", 7, lambda p: mine_n, all_n)
    x_n.start_all()
    all_n[me] = mine_n[...]
    x_n.wait_all()

    for b in range(B):
        norm_f[b * heads : (b + 1) * heads, :] = all_n[b].astype(f32)
    normed = jnp.concatenate(
        [norm_f[pl.ds(h, B, stride=heads), :].astype(bf16) for h in range(heads)], axis=1
    )
    attn_out = jnp.dot(normed, wo_v[...], preferred_element_type=f32)
    res_v[...] = (tok_v[...].astype(f32) + attn_out).astype(bf16)
    my_y, my_c = my_tp // 2, lax.rem(my_tp, 2)
    res_sent = sems.at[9, 0]

    def res_copy(dy, dc):
        peer = lax.rem(my_y + dy, ny) * 2 + lax.rem(my_c + dc, 2)
        return remote(res_v, all_res.at[my_tp], res_sent, res_sem.at[(ny - dy) % ny], "tp", peer)

    for dy, dc in [(0, 1)] + [(d, c) for d in range(ny - 1, 0, -1) for c in range(2)]:
        res_copy(dy, dc).start()
    all_res[my_tp] = res_v[...]

    cw = up_v.shape[2]
    square = lax.broadcasted_iota(jnp.int32, (R, 128), 0) == lax.broadcasted_iota(
        jnp.int32, (R, 128), 1
    )
    chips = [lax.rem(my_y + dy, ny) for dy in range(ny)]
    ats = [rows_of(y * R, R) for y in chips]
    x_sq, x_up, x_act = [], [], []
    for dy, at in enumerate(ats):
        x_sq.append(
            Exchange(
                "kv",
                kv_peers,
                me,
                lambda p, dy=dy: sq_v.at[dy],
                lambda p, dy=dy: got_sq.at[dy, p],
                got_sq.at[dy, pl.ds(0, n - 1)],
                sems.at[11 + 3 * dy],
            )
        )
        for xs, src_of, dst, i in (
            (x_up, lambda p, at=at: up_v.at[p, at], got_up, 12 + 3 * dy),
            (x_act, lambda p, at=at: mine_act.at[at], all_act, 13 + 3 * dy),
        ):
            xs.append(
                Exchange(
                    "kv",
                    kv_peers,
                    me,
                    src_of,
                    lambda p, dst=dst, at=at: dst.at[p, at],
                    dst.at[pl.ds(0, n - 1), at],
                    sems.at[i],
                )
            )

    for dy, (y, at) in enumerate(zip(chips, ats)):
        arrived = all_res.at[pl.ds(0, 2 if dy else 1)]
        remote(arrived, arrived, res_sent, res_sem.at[dy], "tp", tp_peers[0]).wait_recv()
        every = all_res[pl.ds(y * 2, 2)].reshape(R, cols).astype(f32)
        gained = (every * mg_v[...]).astype(bf16)
        row_sq = jnp.sum(every * every, axis=1, keepdims=True)
        sq_v[dy] = jnp.sum(jnp.where(square, row_sq, 0.0), axis=0, keepdims=True)
        up = jnp.dot(gained, wu_v[...], preferred_element_type=f32)
        for p in range(n):
            up_v[p, at] = up[:, p * cw : (p + 1) * cw].astype(bf16)
        for peer in kv_peers:
            x_sq[dy].copy(peer).start()
            x_up[dy].copy(peer).start()
        got_sq[dy, me] = sq_v[dy]
        got_up[me, at] = up_v[me, at]
    for dy, at in enumerate(ats):
        x_sq[dy].wait_all()
        total = got_sq[dy, 0]
        for k in range(1, n):
            total = total + got_sq[dy, k]
        inv_row = lax.rsqrt(total / full_width + norm_eps)
        inv_two = jnp.sum(jnp.where(square, inv_row, 0.0), axis=1, keepdims=True)
        x_up[dy].wait_all()
        total = got_up[0, at].astype(f32)
        for k in range(1, n):
            total = total + got_up[k, at].astype(f32)
        pre = jnp.maximum(total * inv_two, 0.0)
        mine_act[at, :] = (pre * pre).astype(bf16)
        x_act[dy].start_all()
        all_act[me, at] = mine_act[at, :]

    x_down = ex("tp", 10, lambda p: down_v.at[rows_of(p * B, B)], got_down)
    for dy, (y, at) in enumerate(zip(chips, ats)):
        x_act[dy].wait_all()
        act = jnp.concatenate([all_act[k, at] for k in range(n)], axis=1)
        down_v[at, :] = jnp.dot(act, wd_v[...], preferred_element_type=f32).astype(bf16)
        for peer in [y * 2, y * 2 + 1] if dy else [y * 2 + 1 - my_c]:
            x_down.copy(peer).start()
    got_down[my_tp] = down_v[rows_of(my_tp * B, B), :]
    x_down.wait_all()
    total = got_down[0].astype(f32)
    for k in range(1, n_tp):
        total = total + got_down[k].astype(f32)
    mixed[...] = (res_v[...].astype(f32) + total).astype(bf16)

    x_kv2.wait_all()
    sent = all_res.at[pl.ds(0, n_tp - 1)]
    remote(sent, sent, res_sent, res_sem.at[0], "tp", tp_peers[0]).wait_send()
    once = [x_s, x_q, x_kv, x_far, x_near, x_kv2, x_acc, x_stat, x_n, x_down]
    for x in once + x_sq + x_up + x_act:
        x.drain()


def result_kernel(mixed, kv_out, out, new_keys, new_values, sems):
    copies = [
        pltpu.make_async_copy(src, dst, sems.at[i])
        for i, (src, dst) in enumerate(
            ((mixed, out), (kv_out.at[:, 0], new_keys), (kv_out.at[:, 1], new_values))
        )
    ]
    for c in copies:
        c.start()
    for c in copies:
        c.wait()


def shards(
    tokens,
    cache_keys,
    cache_values,
    attn_gain,
    w_query,
    w_key,
    w_value,
    lambdas,
    head_gain,
    w_out,
    mlp_gain,
    w_up,
    w_down,
):
    B, tok_width = tokens.shape
    n = lax.axis_size("kv")
    n_tp = lax.axis_size("tp")
    kv_heads = cache_keys.shape[2]
    comp = cache_keys.shape[3] // 2
    vd = cache_values.shape[3]
    ctx = cache_keys.shape[1]
    heads = lambdas.shape[0]
    span = ctx * kv_heads
    all_rows = B * n_tp
    hidden = w_up.shape[1]
    cw = hidden // n
    lines = 2 * heads
    assert B == n and comp * 2 == 128 and vd == 128
    V = pltpu.VMEM
    scratch = [
        V(tokens.shape, bf16),
        V((1, tok_width), f32),
        V(w_query.shape, bf16),
        V(w_key.shape, bf16),
        V(w_value.shape, bf16),
        V((1, heads), f32),
        V((1, vd), f32),
        V((1, tok_width), f32),
        V((B, span, 128), bf16),
        V((B, span, 128), bf16),
        V(w_out.shape, bf16),
        V(w_up.shape, bf16),
        V(w_down.shape, bf16),
        DMA((11,)),
        DMA,
        DMA,
        V((B * heads, 128), f32),
        V((B, 1, 128), f32),
        V((B * 8, 128), f32),
        V((n, heads, 128), f32),
        V((n, 1, 128), f32),
        V((n, 8, 128), f32),
        V((heads, 128), bf16),
        V((2, kv_heads, 128), bf16),
        V((n, heads, 128), bf16),
        V((n, lines, vd), bf16),
        V((n, 2, 128), f32),
        V((n, lines, vd), bf16),
        V((n, 2, 128), f32),
        V((heads, vd), bf16),
        V((n, heads, vd), bf16),
        V((B * heads, vd), f32),
        V((B, tok_width), bf16),
        V((n_tp, B, tok_width), bf16),
        V((n_tp // 2, 1, 128), f32),
        V((n_tp // 2, n, 1, 128), f32),
        V((n, all_rows, cw), bf16),
        V((n, all_rows, cw), bf16),
        V((all_rows, cw), bf16),
        V((n, all_rows, cw), bf16),
        V((all_rows, tok_width), bf16),
        V((n_tp, B, tok_width), bf16),
        DMA((11 + 3 * (n_tp // 2), 2)),
        DMA((n_tp // 2,)),
    ]
    mixed, kv_out = pl.pallas_call(
        functools.partial(
            layer_kernel, n, n_tp, kv_heads, tok_width * n, ctx * n, comp ** (-0.5)
        ),
        out_shape=(
            jax.ShapeDtypeStruct((B, tok_width), bf16),
            jax.ShapeDtypeStruct((n, 2, kv_heads, 128), bf16),
        ),
        in_specs=[HBM] * 13,
        out_specs=(VM, VM),
        scratch_shapes=scratch,
        compiler_params=pltpu.CompilerParams(
            collective_id=0, has_side_effects=True, vmem_limit_bytes=48 * 1024 * 1024
        ),
    )(
        *[
            pltpu.with_memory_space_constraint(x, pltpu.HBM)
            for x in (
                tokens,
                cache_keys.reshape(B, span, 128),
                cache_values.reshape(B, span, vd),
                attn_gain.reshape(1, tok_width),
                w_query,
                w_key,
                w_value,
                lambdas.reshape(1, heads),
                head_gain.reshape(1, vd),
                w_out,
                mlp_gain.reshape(1, tok_width),
                w_up,
                w_down,
            )
        ]
    )
    return pl.pallas_call(
        result_kernel,
        out_shape=(
            jax.ShapeDtypeStruct(mixed.shape, bf16),
            jax.ShapeDtypeStruct((n, kv_heads, 128), bf16),
            jax.ShapeDtypeStruct((n, kv_heads, 128), bf16),
        ),
        in_specs=[VM, VM],
        out_specs=(HBM, HBM, HBM),
        scratch_shapes=[DMA((3,))],
        compiler_params=pltpu.CompilerParams(vmem_limit_bytes=1024 * 1024),
    )(mixed, kv_out)


def solution(mesh):
    in_specs = (
        P("tp", "kv"),
        P("tp", "kv", None, None),
        P("tp", "kv", None, None),
        P("kv"),
        P("kv", None),
        P("kv", None),
        P("kv", None),
        P(),
        P(),
        P(None, "kv"),
        P("kv"),
        P("kv", "tp"),
        P("tp", "kv"),
    )
    out_specs = (P("tp", "kv"), P("tp", None, None), P("tp", None, None))
    return jax.shard_map(shards, mesh=mesh, in_specs=in_specs, out_specs=out_specs, check_vma=False)
```

```python
import functools

import jax
import jax.numpy as jnp
from jax import lax
from jax.experimental import pallas as pl
from jax.experimental.pallas import tpu as pltpu
from jax.sharding import PartitionSpec as P

norm_eps = 1e-06
f32 = jnp.float32
bf16 = jnp.bfloat16
VM = pl.BlockSpec(memory_space=pltpu.VMEM)
HBM = pl.BlockSpec(memory_space=pltpu.HBM)
DMA = pltpu.SemaphoreType.DMA
NT = (((1,), (1,)), ((), ()))
UNROLL = 4
AHEAD = 2
BEHIND = 1


def remote(src, dst, send, recv, axis, peer):
    return pltpu.make_async_remote_copy(
        src_ref=src,
        dst_ref=dst,
        send_sem=send,
        recv_sem=recv,
        device_id={axis: peer},
        device_id_type=pl.DeviceIdType.MESH,
    )


class Exchange:
    def __init__(self, axis, peers, me, src_of, dst_of, all_dst, sems):
        self.axis, self.peers, self.me = axis, peers, me
        self.src_of, self.dst_of, self.all_dst = src_of, dst_of, all_dst
        self.send, self.recv = sems.at[0], sems.at[1]

    def copy(self, peer):
        return remote(
            self.src_of(peer), self.dst_of(self.me), self.send, self.recv, self.axis, peer
        )

    def start_all(self):
        for peer in self.peers:
            self.copy(peer).start()

    def everything(self):
        return remote(self.all_dst, self.all_dst, self.send, self.recv, self.axis, self.peers[0])

    def wait_all(self):
        self.everything().wait_recv()

    def drain(self):
        self.everything().wait_send()


def offsets(outer, inner, wrap_inner):
    def far(d, size, wrap):
        return min(d, size - d) if wrap else d % 2

    every = [(a, b) for a in range(outer) for b in range(inner)]
    every.sort(key=lambda o: -(far(o[0], outer, True) + far(o[1], inner, wrap_inner) / 1.5))
    return every


def rows_of(start, size):
    return pl.ds(pl.multiple_of(start, size), size)


def layer_kernel(
    n,
    n_tp,
    kv_heads,
    full_width,
    ctx_total,
    scale,
    tokens,
    keys,
    values,
    attn_gain,
    w_query,
    w_key,
    w_value,
    lambdas,
    head_gain,
    w_out,
    mlp_gain,
    w_up,
    w_down,
    mixed,
    kv_out,
    tok_v,
    ag_v,
    wq_v,
    wk_v,
    wv_v,
    lam_v,
    hg_v,
    mg_v,
    kbuf,
    vbuf,
    wo_v,
    wu_v,
    wd_v,
    lsem,
    ksem,
    vsem,
    part_q,
    part_s,
    part_kv,
    got_q,
    got_s,
    got_kv,
    mine_q,
    mine_kv,
    all_q,
    acc,
    stat,
    gacc,
    gstat,
    mine_n,
    all_n,
    norm_f,
    res_v,
    all_res,
    sq_v,
    got_sq,
    up_v,
    got_up,
    mine_act,
    all_act,
    down_v,
    got_down,
    sems,
    res_sem,
):
    me = lax.axis_index("kv")
    my_tp = lax.axis_index("tp")
    B = tokens.shape[0]
    heads = got_q.shape[1]
    half = heads // kv_heads
    lines = 2 * heads
    span = keys.shape[1]
    cols = tok_v.shape[1]
    all_rows = B * n_tp
    R = 2 * B
    groups = span // 128

    def order(at, outer, inner, wrap_inner):
        a, b = at // inner, lax.rem(at, inner)
        return [
            lax.rem(a + da, outer) * inner + lax.rem(b + db, inner)
            for da, db in offsets(outer, inner, wrap_inner)
        ]

    side = int(n**0.5)
    ny = n_tp // 2
    kv_order = order(me, side, side, True)
    kv_peers = kv_order[:-1]
    near_peers, far_peers = kv_order[-5:-1], kv_order[:-5]
    tp_peers = order(my_tp, ny, 2, False)[:-1]

    def ex(axis, i, src_of, dst, peers=None):
        every, at = (kv_peers, me) if axis == "kv" else (tp_peers, my_tp)
        peers = every if peers is None else peers
        return Exchange(
            axis, peers, at, src_of, lambda p: dst.at[p], dst.at[pl.ds(0, len(peers))], sems.at[i]
        )

    first = [(tokens, tok_v), (attn_gain, ag_v), (w_query, wq_v), (w_key, wk_v), (w_value, wv_v)]
    later = [
        (lambdas, lam_v),
        (head_gain, hg_v),
        (w_out, wo_v),
        (mlp_gain, mg_v),
        (w_up, wu_v),
        (w_down, wd_v),
    ]
    first = [pltpu.make_async_copy(a, b, lsem.at[i]) for i, (a, b) in enumerate(first)]
    later = [pltpu.make_async_copy(a, b, lsem.at[len(first) + i]) for i, (a, b) in enumerate(later)]
    for c in first:
        c.start()
    barrier = pltpu.get_barrier_semaphore()
    for axis, peers in (("kv", kv_peers), ("tp", tp_peers)):
        for peer in peers:
            pl.semaphore_signal(
                barrier, inc=1, device_id={axis: peer}, device_id_type=pl.DeviceIdType.MESH
            )
    for c in first:
        c.wait()

    for src, dst, sem in ((keys, kbuf, ksem), (values, vbuf, vsem)):
        for b in kv_order:
            pltpu.make_async_copy(src.at[b], dst.at[b], sem).start()
    for c in later:
        c.start()

    tok_f = tok_v[...].astype(f32)
    scaled = (tok_f * ag_v[...]).astype(bf16)
    squares = jnp.broadcast_to(jnp.sum(tok_f * tok_f, axis=1, keepdims=True), (B, 128))
    for r in range(B):
        part_s[r] = squares[r : r + 1]
    product = jnp.dot(scaled, wq_v[...], preferred_element_type=f32)
    for h in range(heads):
        part_q[pl.ds(h, B, stride=heads), :] = product[:, h * 128 : (h + 1) * 128]
    pieces = 0
    for w in (wk_v, wv_v):
        product = jnp.dot(scaled, w[...], preferred_element_type=f32)
        for h in range(product.shape[1] // 128):
            part_kv[pl.ds(pieces, B, stride=8), :] = product[:, h * 128 : (h + 1) * 128]
            pieces += 1
    for h in range(pieces, 8):
        part_kv[pl.ds(h, B, stride=8), :] = jnp.zeros((B, 128), f32)

    x_q = ex("kv", 0, lambda p: part_q.at[rows_of(p * heads, heads)], got_q)
    x_s = ex("kv", 1, lambda p: part_s.at[p], got_s)
    x_kv = ex("kv", 2, lambda p: part_kv.at[rows_of(p * 8, 8)], got_kv)
    pl.semaphore_wait(barrier, n - 1 + n_tp - 1)
    for peer in kv_peers:
        x_s.copy(peer).start()
        x_q.copy(peer).start()
    x_kv.start_all()
    got_q[me] = part_q[rows_of(me * heads, heads), :]
    got_s[me] = part_s[me]
    got_kv[me] = part_kv[rows_of(me * 8, 8), :]
    x_s.wait_all()
    total = got_s[0]
    for k in range(1, n):
        total = total + got_s[k]
    inv_one = lax.rsqrt(total / full_width + norm_eps)
    x_q.wait_all()
    total = got_q[0]
    for k in range(1, n):
        total = total + got_q[k]
    query = (total * inv_one).astype(bf16).astype(f32) * scale
    mine_q[...] = query.astype(bf16)
    x_far = ex("kv", 3, lambda p: mine_q, all_q, far_peers)
    x_near = ex("kv", 8, lambda p: mine_q, all_q, near_peers)
    x_far.start_all()
    x_near.start_all()
    all_q[me] = mine_q[...]
    x_kv.wait_all()
    total = got_kv[0]
    for k in range(1, n):
        total = total + got_kv[k]
    new_kv = (total * inv_one).astype(bf16)
    for i in range(2):
        mine_kv[i] = new_kv[i * kv_heads : (i + 1) * kv_heads]
    x_kv2 = ex("kv", 4, lambda p: mine_kv, kv_out)
    x_kv2.start_all()
    kv_out[me] = mine_kv[...]

    lane = lax.broadcasted_iota(jnp.int32, (heads, 128), 1)
    even = lax.rem(lane, 2) == 0
    low = lane < 64
    diag = lax.broadcasted_iota(jnp.int32, (lines, 128), 1) == lax.broadcasted_iota(
        jnp.int32, (lines, 128), 0
    )

    x_acc = ex("kv", 5, lambda p: acc.at[p], gacc)
    x_stat = ex("kv", 6, lambda p: stat.at[p], gstat)

    def scores_of(b):
        q = all_q[b].astype(f32)
        lo = jnp.where(low, q, 0.0)
        hi = jnp.where(low, 0.0, q)
        q_lines = jnp.concatenate([lo[:half], hi[:half], lo[half:], hi[half:]], axis=0).astype(bf16)
        return lax.dot_general(q_lines, kbuf[b], NT, preferred_element_type=f32)

    def softmax_of(s):
        m = [
            jnp.where(even, s[:heads, c * 128 : (c + 1) * 128], s[heads:, c * 128 : (c + 1) * 128])
            for c in range(groups)
        ]
        top = m[0]
        for c in range(1, groups):
            top = jnp.maximum(top, m[c])
        top0 = jnp.max(jnp.where(even, top, -jnp.inf), axis=1, keepdims=True)
        top1 = jnp.max(jnp.where(even, -jnp.inf, top), axis=1, keepdims=True)
        top = jnp.where(even, top0, top1)
        m = [jnp.exp(x - top) for x in m]
        total = m[0]
        for c in range(1, groups):
            total = total + m[c]
        tot0 = jnp.sum(jnp.where(even, total, 0.0), axis=1, keepdims=True)
        tot1 = jnp.sum(jnp.where(even, 0.0, total), axis=1, keepdims=True)
        e = jnp.concatenate(
            [
                jnp.concatenate([jnp.where(even, x, 0.0).astype(bf16) for x in m], axis=1),
                jnp.concatenate([jnp.where(even, 0.0, x).astype(bf16) for x in m], axis=1),
            ],
            axis=0,
        )
        tops = jnp.concatenate([top0, top1], axis=0)
        tots = jnp.concatenate([tot0, tot1], axis=0)
        row0 = jnp.sum(jnp.where(diag, tops, 0.0), axis=0, keepdims=True)
        row1 = jnp.sum(jnp.where(diag, tots, 0.0), axis=0, keepdims=True)
        return e, jnp.concatenate([row0, row1], axis=0)

    def attend(bs, send=True):
        s, e = {}, {}
        for i in range(-AHEAD, len(bs) + BEHIND):
            if i + AHEAD < len(bs):
                s[i + AHEAD] = scores_of(bs[i + AHEAD])
            if 0 <= i < len(bs):
                e[i], stat[bs[i]] = softmax_of(s.pop(i))
            if i >= BEHIND:
                b = bs[i - BEHIND]
                acc[b] = jnp.dot(e.pop(i - BEHIND), vbuf[b], preferred_element_type=f32).astype(bf16)
        for b in bs if send else ():
            x_acc.copy(b).start()
            x_stat.copy(b).start()

    pltpu.make_async_copy(keys, kbuf, ksem).wait()
    pltpu.make_async_copy(values, vbuf, vsem).wait()
    attend([me], send=False)
    x_near.wait_all()
    attend(near_peers)
    x_far.wait_all()
    for i in range(0, len(far_peers), UNROLL):
        attend(far_peers[i : i + UNROLL])
    gacc[me] = acc[me]
    gstat[me] = stat[me]
    for c in later:
        c.wait()
    lam = jnp.broadcast_to(lam_v[...], (heads, heads))
    lam = jnp.sum(
        jnp.where(
            lax.broadcasted_iota(jnp.int32, (heads, heads), 0)
            == lax.broadcasted_iota(jnp.int32, (heads, heads), 1),
            lam,
            0.0,
        ),
        axis=1,
        keepdims=True,
    )
    x_stat.wait_all()
    tops = [gstat[k][0:1] for k in range(n)]
    peak = tops[0]
    for t in tops[1:]:
        peak = jnp.maximum(peak, t)
    facs = [jnp.exp(t - peak) for t in tops]
    total = facs[0] * gstat[0][1:2]
    for k in range(1, n):
        total = total + facs[k] * gstat[k][1:2]
    table = jnp.transpose(
        jnp.concatenate(facs + [jnp.broadcast_to(total, (8, 128))], axis=0)
    )
    x_acc.wait_all()
    merged = table[:lines, 0:1] * gacc[0].astype(f32)
    for k in range(1, n):
        merged = merged + table[:lines, k : k + 1] * gacc[k].astype(f32)
    ratio = merged / table[:lines, n : n + 1]
    normed = []
    for g in range(kv_heads):
        base = g * 2 * half
        head = ratio[base : base + half] - lam[g * half : (g + 1) * half] * ratio[base + half : base + 2 * half]
        mean_sq = jnp.mean(head * head, axis=1, keepdims=True)
        normed.append(head * lax.rsqrt(mean_sq + 1.0 / ctx_total) * hg_v[...])
    mine_n[...] = jnp.concatenate(normed, axis=0).astype(bf16)
    x_n = ex("kv", 7, lambda p: mine_n, all_n)
    x_n.start_all()
    all_n[me] = mine_n[...]
    x_n.wait_all()

    for b in range(B):
        norm_f[b * heads : (b + 1) * heads, :] = all_n[b].astype(f32)
    normed = jnp.concatenate(
        [norm_f[pl.ds(h, B, stride=heads), :].astype(bf16) for h in range(heads)], axis=1
    )
    attn_out = jnp.dot(normed, wo_v[...], preferred_element_type=f32)
    res_v[...] = (tok_v[...].astype(f32) + attn_out).astype(bf16)
    my_y, my_c = my_tp // 2, lax.rem(my_tp, 2)
    res_sent = sems.at[9, 0]

    def res_copy(dy, dc):
        peer = lax.rem(my_y + dy, ny) * 2 + lax.rem(my_c + dc, 2)
        return remote(res_v, all_res.at[my_tp], res_sent, res_sem.at[(ny - dy) % ny], "tp", peer)

    for dy, dc in [(0, 1)] + [(d, c) for d in range(ny - 1, 0, -1) for c in range(2)]:
        res_copy(dy, dc).start()
    all_res[my_tp] = res_v[...]

    cw = up_v.shape[2]
    square = lax.broadcasted_iota(jnp.int32, (R, 128), 0) == lax.broadcasted_iota(
        jnp.int32, (R, 128), 1
    )
    chips = [lax.rem(my_y + dy, ny) for dy in range(ny)]
    ats = [rows_of(y * R, R) for y in chips]
    x_sq, x_up, x_act = [], [], []
    for dy, at in enumerate(ats):
        x_sq.append(
            Exchange(
                "kv",
                kv_peers,
                me,
                lambda p, dy=dy: sq_v.at[dy],
                lambda p, dy=dy: got_sq.at[dy, p],
                got_sq.at[dy, pl.ds(0, n - 1)],
                sems.at[11 + 3 * dy],
            )
        )
        for xs, src_of, dst, i in (
            (x_up, lambda p, at=at: up_v.at[p, at], got_up, 12 + 3 * dy),
            (x_act, lambda p, at=at: mine_act.at[at], all_act, 13 + 3 * dy),
        ):
            xs.append(
                Exchange(
                    "kv",
                    kv_peers,
                    me,
                    src_of,
                    lambda p, dst=dst, at=at: dst.at[p, at],
                    dst.at[pl.ds(0, n - 1), at],
                    sems.at[i],
                )
            )

    for dy, (y, at) in enumerate(zip(chips, ats)):
        arrived = all_res.at[pl.ds(0, 2 if dy else 1)]
        remote(arrived, arrived, res_sent, res_sem.at[dy], "tp", tp_peers[0]).wait_recv()
        every = all_res[pl.ds(y * 2, 2)].reshape(R, cols).astype(f32)
        gained = (every * mg_v[...]).astype(bf16)
        row_sq = jnp.sum(every * every, axis=1, keepdims=True)
        sq_v[dy] = jnp.sum(jnp.where(square, row_sq, 0.0), axis=0, keepdims=True)
        up = jnp.dot(gained, wu_v[...], preferred_element_type=f32)
        for p in range(n):
            up_v[p, at] = up[:, p * cw : (p + 1) * cw].astype(bf16)
        for peer in kv_peers:
            x_sq[dy].copy(peer).start()
            x_up[dy].copy(peer).start()
        got_sq[dy, me] = sq_v[dy]
        got_up[me, at] = up_v[me, at]
    for dy, at in enumerate(ats):
        x_sq[dy].wait_all()
        total = got_sq[dy, 0]
        for k in range(1, n):
            total = total + got_sq[dy, k]
        inv_row = lax.rsqrt(total / full_width + norm_eps)
        inv_two = jnp.sum(jnp.where(square, inv_row, 0.0), axis=1, keepdims=True)
        x_up[dy].wait_all()
        total = got_up[0, at].astype(f32)
        for k in range(1, n):
            total = total + got_up[k, at].astype(f32)
        pre = jnp.maximum(total * inv_two, 0.0)
        mine_act[at, :] = (pre * pre).astype(bf16)
        x_act[dy].start_all()
        all_act[me, at] = mine_act[at, :]

    x_down = ex("tp", 10, lambda p: down_v.at[rows_of(p * B, B)], got_down)
    for dy, (y, at) in enumerate(zip(chips, ats)):
        x_act[dy].wait_all()
        act = jnp.concatenate([all_act[k, at] for k in range(n)], axis=1)
        down_v[at, :] = jnp.dot(act, wd_v[...], preferred_element_type=f32).astype(bf16)
        for peer in [y * 2, y * 2 + 1] if dy else [y * 2 + 1 - my_c]:
            x_down.copy(peer).start()
    got_down[my_tp] = down_v[rows_of(my_tp * B, B), :]
    x_down.wait_all()
    total = got_down[0].astype(f32)
    for k in range(1, n_tp):
        total = total + got_down[k].astype(f32)
    mixed[...] = (res_v[...].astype(f32) + total).astype(bf16)

    x_kv2.wait_all()
    sent = all_res.at[pl.ds(0, n_tp - 1)]
    remote(sent, sent, res_sent, res_sem.at[0], "tp", tp_peers[0]).wait_send()
    once = [x_s, x_q, x_kv, x_far, x_near, x_kv2, x_acc, x_stat, x_n, x_down]
    for x in once + x_sq + x_up + x_act:
        x.drain()


def result_kernel(mixed, kv_out, out, new_keys, new_values, sems):
    copies = [
        pltpu.make_async_copy(src, dst, sems.at[i])
        for i, (src, dst) in enumerate(
            ((mixed, out), (kv_out.at[:, 0], new_keys), (kv_out.at[:, 1], new_values))
        )
    ]
    for c in copies:
        c.start()
    for c in copies:
        c.wait()


def shards(
    tokens,
    cache_keys,
    cache_values,
    attn_gain,
    w_query,
    w_key,
    w_value,
    lambdas,
    head_gain,
    w_out,
    mlp_gain,
    w_up,
    w_down,
):
    B, tok_width = tokens.shape
    n = lax.axis_size("kv")
    n_tp = lax.axis_size("tp")
    kv_heads = cache_keys.shape[2]
    comp = cache_keys.shape[3] // 2
    vd = cache_values.shape[3]
    ctx = cache_keys.shape[1]
    heads = lambdas.shape[0]
    span = ctx * kv_heads
    all_rows = B * n_tp
    hidden = w_up.shape[1]
    cw = hidden // n
    lines = 2 * heads
    assert B == n and comp * 2 == 128 and vd == 128
    V = pltpu.VMEM
    scratch = [
        V(tokens.shape, bf16),
        V((1, tok_width), f32),
        V(w_query.shape, bf16),
        V(w_key.shape, bf16),
        V(w_value.shape, bf16),
        V((1, heads), f32),
        V((1, vd), f32),
        V((1, tok_width), f32),
        V((B, span, 128), bf16),
        V((B, span, 128), bf16),
        V(w_out.shape, bf16),
        V(w_up.shape, bf16),
        V(w_down.shape, bf16),
        DMA((11,)),
        DMA,
        DMA,
        V((B * heads, 128), f32),
        V((B, 1, 128), f32),
        V((B * 8, 128), f32),
        V((n, heads, 128), f32),
        V((n, 1, 128), f32),
        V((n, 8, 128), f32),
        V((heads, 128), bf16),
        V((2, kv_heads, 128), bf16),
        V((n, heads, 128), bf16),
        V((n, lines, vd), bf16),
        V((n, 2, 128), f32),
        V((n, lines, vd), bf16),
        V((n, 2, 128), f32),
        V((heads, vd), bf16),
        V((n, heads, vd), bf16),
        V((B * heads, vd), f32),
        V((B, tok_width), bf16),
        V((n_tp, B, tok_width), bf16),
        V((n_tp // 2, 1, 128), f32),
        V((n_tp // 2, n, 1, 128), f32),
        V((n, all_rows, cw), bf16),
        V((n, all_rows, cw), bf16),
        V((all_rows, cw), bf16),
        V((n, all_rows, cw), bf16),
        V((all_rows, tok_width), bf16),
        V((n_tp, B, tok_width), bf16),
        DMA((11 + 3 * (n_tp // 2), 2)),
        DMA((n_tp // 2,)),
    ]
    mixed, kv_out = pl.pallas_call(
        functools.partial(
            layer_kernel, n, n_tp, kv_heads, tok_width * n, ctx * n, comp ** (-0.5)
        ),
        out_shape=(
            jax.ShapeDtypeStruct((B, tok_width), bf16),
            jax.ShapeDtypeStruct((n, 2, kv_heads, 128), bf16),
        ),
        in_specs=[HBM] * 13,
        out_specs=(VM, VM),
        scratch_shapes=scratch,
        compiler_params=pltpu.CompilerParams(
            collective_id=0, has_side_effects=True, vmem_limit_bytes=48 * 1024 * 1024
        ),
    )(
        *[
            pltpu.with_memory_space_constraint(x, pltpu.HBM)
            for x in (
                tokens,
                cache_keys.reshape(B, span, 128),
                cache_values.reshape(B, span, vd),
                attn_gain.reshape(1, tok_width),
                w_query,
                w_key,
                w_value,
                lambdas.reshape(1, heads),
                head_gain.reshape(1, vd),
                w_out,
                mlp_gain.reshape(1, tok_width),
                w_up,
                w_down,
            )
        ]
    )
    return pl.pallas_call(
        result_kernel,
        out_shape=(
            jax.ShapeDtypeStruct(mixed.shape, bf16),
            jax.ShapeDtypeStruct((n, kv_heads, 128), bf16),
            jax.ShapeDtypeStruct((n, kv_heads, 128), bf16),
        ),
        in_specs=[VM, VM],
        out_specs=(HBM, HBM, HBM),
        scratch_shapes=[DMA((3,))],
        compiler_params=pltpu.CompilerParams(vmem_limit_bytes=1024 * 1024),
    )(mixed, kv_out)


def solution(mesh):
    in_specs = (
        P("tp", "kv"),
        P("tp", "kv", None, None),
        P("tp", "kv", None, None),
        P("kv"),
        P("kv", None),
        P("kv", None),
        P("kv", None),
        P(),
        P(),
        P(None, "kv"),
        P("kv"),
        P("kv", "tp"),
        P("tp", "kv"),
    )
    out_specs = (P("tp", "kv"), P("tp", None, None), P("tp", None, None))
    return jax.shard_map(shards, mesh=mesh, in_specs=in_specs, out_specs=out_specs, check_vma=False)
```

```python
import functools

import jax
import jax.numpy as jnp
from jax import lax
from jax.experimental import pallas as pl
from jax.experimental.pallas import tpu as pltpu
from jax.sharding import PartitionSpec as P

norm_eps = 1e-06
f32 = jnp.float32
bf16 = jnp.bfloat16
VM = pl.BlockSpec(memory_space=pltpu.VMEM)
HBM = pl.BlockSpec(memory_space=pltpu.HBM)
DMA = pltpu.SemaphoreType.DMA
NT = (((1,), (1,)), ((), ()))
UNROLL = 4
AHEAD = 2
FLIPPED = 8
BEHIND = 1


def remote(src, dst, send, recv, axis, peer):
    return pltpu.make_async_remote_copy(
        src_ref=src,
        dst_ref=dst,
        send_sem=send,
        recv_sem=recv,
        device_id={axis: peer},
        device_id_type=pl.DeviceIdType.MESH,
    )


class Exchange:
    def __init__(self, axis, peers, me, src_of, dst_of, all_dst, sems):
        self.axis, self.peers, self.me = axis, peers, me
        self.src_of, self.dst_of, self.all_dst = src_of, dst_of, all_dst
        self.send, self.recv = sems.at[0], sems.at[1]

    def copy(self, peer):
        return remote(
            self.src_of(peer), self.dst_of(self.me), self.send, self.recv, self.axis, peer
        )

    def start_all(self):
        for peer in self.peers:
            self.copy(peer).start()

    def everything(self):
        return remote(self.all_dst, self.all_dst, self.send, self.recv, self.axis, self.peers[0])

    def wait_all(self):
        self.everything().wait_recv()

    def drain(self):
        self.everything().wait_send()


def offsets(outer, inner, wrap_inner):
    def far(d, size, wrap):
        return min(d, size - d) if wrap else d % 2

    every = [(a, b) for a in range(outer) for b in range(inner)]
    every.sort(key=lambda o: -(far(o[0], outer, True) + far(o[1], inner, wrap_inner) / 1.5))
    return every


def rows_of(start, size):
    return pl.ds(pl.multiple_of(start, size), size)


def layer_kernel(
    n,
    n_tp,
    kv_heads,
    full_width,
    ctx_total,
    scale,
    tokens,
    keys,
    values,
    attn_gain,
    w_query,
    w_key,
    w_value,
    lambdas,
    head_gain,
    w_out,
    mlp_gain,
    w_up,
    w_down,
    mixed,
    kv_out,
    tok_v,
    ag_v,
    wq_v,
    wk_v,
    wv_v,
    lam_v,
    hg_v,
    mg_v,
    kbuf,
    vbuf,
    wo_v,
    wu_v,
    wd_v,
    lsem,
    ksem,
    vsem,
    part_q,
    part_s,
    part_kv,
    got_q,
    got_s,
    got_kv,
    mine_q,
    mine_kv,
    all_q,
    acc,
    stat,
    gacc,
    gstat,
    mine_n,
    all_n,
    norm_f,
    res_v,
    all_res,
    sq_v,
    got_sq,
    up_v,
    got_up,
    mine_act,
    all_act,
    down_v,
    got_down,
    sems,
    res_sem,
    flipped,
):
    me = lax.axis_index("kv")
    my_tp = lax.axis_index("tp")
    B = tokens.shape[0]
    heads = got_q.shape[1]
    half = heads // kv_heads
    lines = 2 * heads
    span = keys.shape[1]
    cols = tok_v.shape[1]
    all_rows = B * n_tp
    R = 2 * B
    groups = span // 128

    def order(at, outer, inner, wrap_inner):
        a, b = at // inner, lax.rem(at, inner)
        return [
            lax.rem(a + da, outer) * inner + lax.rem(b + db, inner)
            for da, db in offsets(outer, inner, wrap_inner)
        ]

    side = int(n**0.5)
    ny = n_tp // 2
    kv_order = order(me, side, side, True)
    kv_peers = kv_order[:-1]
    near_peers, far_peers = kv_order[-5:-1], kv_order[:-5]
    tp_peers = order(my_tp, ny, 2, False)[:-1]

    def ex(axis, i, src_of, dst, peers=None):
        every, at = (kv_peers, me) if axis == "kv" else (tp_peers, my_tp)
        peers = every if peers is None else peers
        return Exchange(
            axis, peers, at, src_of, lambda p: dst.at[p], dst.at[pl.ds(0, len(peers))], sems.at[i]
        )

    first = [(tokens, tok_v), (attn_gain, ag_v), (w_query, wq_v), (w_key, wk_v), (w_value, wv_v)]
    later = [
        (lambdas, lam_v),
        (head_gain, hg_v),
        (w_out, wo_v),
        (mlp_gain, mg_v),
        (w_up, wu_v),
        (w_down, wd_v),
    ]
    first = [pltpu.make_async_copy(a, b, lsem.at[i]) for i, (a, b) in enumerate(first)]
    later = [pltpu.make_async_copy(a, b, lsem.at[len(first) + i]) for i, (a, b) in enumerate(later)]
    for c in first:
        c.start()
    barrier = pltpu.get_barrier_semaphore()
    for axis, peers in (("kv", kv_peers), ("tp", tp_peers)):
        for peer in peers:
            pl.semaphore_signal(
                barrier, inc=1, device_id={axis: peer}, device_id_type=pl.DeviceIdType.MESH
            )
    for c in first:
        c.wait()

    for i, b in enumerate(kv_order):
        pltpu.make_async_copy(keys.at[b], kbuf.at[b], ksem.at[i // FLIPPED]).start()
    for b in kv_order:
        pltpu.make_async_copy(values.at[b], vbuf.at[b], vsem).start()

    def keys_wait(i):
        first, size = i * FLIPPED, min(FLIPPED, B - i * FLIPPED)
        at = pl.ds(first, size)
        pltpu.make_async_copy(keys.at[at], kbuf.at[at], ksem.at[i]).wait()

    eye = jnp.where(
        lax.broadcasted_iota(jnp.int32, (128, 128), 0)
        == lax.broadcasted_iota(jnp.int32, (128, 128), 1),
        1.0,
        0.0,
    ).astype(bf16)

    def flip():
        keys_wait(0)
        for i in range(FLIPPED):
            flipped[i] = lax.dot_general(
                eye, kbuf[kv_order[i]], NT, preferred_element_type=f32
            ).astype(bf16)

    for c in later:
        c.start()

    tok_f = tok_v[...].astype(f32)
    scaled = (tok_f * ag_v[...]).astype(bf16)
    squares = jnp.broadcast_to(jnp.sum(tok_f * tok_f, axis=1, keepdims=True), (B, 128))
    for r in range(B):
        part_s[r] = squares[r : r + 1]
    product = jnp.dot(scaled, wq_v[...], preferred_element_type=f32)
    for h in range(heads):
        part_q[pl.ds(h, B, stride=heads), :] = product[:, h * 128 : (h + 1) * 128]
    pieces = 0
    for w in (wk_v, wv_v):
        product = jnp.dot(scaled, w[...], preferred_element_type=f32)
        for h in range(product.shape[1] // 128):
            part_kv[pl.ds(pieces, B, stride=8), :] = product[:, h * 128 : (h + 1) * 128]
            pieces += 1
    for h in range(pieces, 8):
        part_kv[pl.ds(h, B, stride=8), :] = jnp.zeros((B, 128), f32)

    x_q = ex("kv", 0, lambda p: part_q.at[rows_of(p * heads, heads)], got_q)
    x_s = ex("kv", 1, lambda p: part_s.at[p], got_s)
    x_kv = ex("kv", 2, lambda p: part_kv.at[rows_of(p * 8, 8)], got_kv)
    pl.semaphore_wait(barrier, n - 1 + n_tp - 1)
    for peer in kv_peers:
        x_s.copy(peer).start()
        x_q.copy(peer).start()
    x_kv.start_all()
    got_q[me] = part_q[rows_of(me * heads, heads), :]
    got_s[me] = part_s[me]
    got_kv[me] = part_kv[rows_of(me * 8, 8), :]
    flip()
    x_s.wait_all()
    total = got_s[0]
    for k in range(1, n):
        total = total + got_s[k]
    inv_one = lax.rsqrt(total / full_width + norm_eps)
    x_q.wait_all()
    total = got_q[0]
    for k in range(1, n):
        total = total + got_q[k]
    query = (total * inv_one).astype(bf16).astype(f32) * scale
    mine_q[...] = query.astype(bf16)
    x_far = ex("kv", 3, lambda p: mine_q, all_q, far_peers)
    x_near = ex("kv", 8, lambda p: mine_q, all_q, near_peers)
    x_far.start_all()
    x_near.start_all()
    all_q[me] = mine_q[...]
    x_kv.wait_all()
    total = got_kv[0]
    for k in range(1, n):
        total = total + got_kv[k]
    new_kv = (total * inv_one).astype(bf16)
    for i in range(2):
        mine_kv[i] = new_kv[i * kv_heads : (i + 1) * kv_heads]
    x_kv2 = ex("kv", 4, lambda p: mine_kv, kv_out)
    x_kv2.start_all()
    kv_out[me] = mine_kv[...]

    lane = lax.broadcasted_iota(jnp.int32, (heads, 128), 1)
    even = lax.rem(lane, 2) == 0
    low = lane < 64
    diag = lax.broadcasted_iota(jnp.int32, (lines, 128), 1) == lax.broadcasted_iota(
        jnp.int32, (lines, 128), 0
    )

    x_acc = ex("kv", 5, lambda p: acc.at[p], gacc)
    x_stat = ex("kv", 6, lambda p: stat.at[p], gstat)

    def scores_of(b):
        q = all_q[b].astype(f32)
        lo = jnp.where(low, q, 0.0)
        hi = jnp.where(low, 0.0, q)
        q_lines = jnp.concatenate([lo[:half], hi[:half], lo[half:], hi[half:]], axis=0).astype(bf16)
        for i in range(FLIPPED):
            if b is kv_order[i]:
                return jnp.dot(q_lines, flipped[i], preferred_element_type=f32)
        return lax.dot_general(q_lines, kbuf[b], NT, preferred_element_type=f32)

    def softmax_of(s):
        m = [
            jnp.where(even, s[:heads, c * 128 : (c + 1) * 128], s[heads:, c * 128 : (c + 1) * 128])
            for c in range(groups)
        ]
        top = m[0]
        for c in range(1, groups):
            top = jnp.maximum(top, m[c])
        top0 = jnp.max(jnp.where(even, top, -jnp.inf), axis=1, keepdims=True)
        top1 = jnp.max(jnp.where(even, -jnp.inf, top), axis=1, keepdims=True)
        top = jnp.where(even, top0, top1)
        m = [jnp.exp(x - top) for x in m]
        total = m[0]
        for c in range(1, groups):
            total = total + m[c]
        tot0 = jnp.sum(jnp.where(even, total, 0.0), axis=1, keepdims=True)
        tot1 = jnp.sum(jnp.where(even, 0.0, total), axis=1, keepdims=True)
        e = jnp.concatenate(
            [
                jnp.concatenate([jnp.where(even, x, 0.0).astype(bf16) for x in m], axis=1),
                jnp.concatenate([jnp.where(even, 0.0, x).astype(bf16) for x in m], axis=1),
            ],
            axis=0,
        )
        tops = jnp.concatenate([top0, top1], axis=0)
        tots = jnp.concatenate([tot0, tot1], axis=0)
        row0 = jnp.sum(jnp.where(diag, tops, 0.0), axis=0, keepdims=True)
        row1 = jnp.sum(jnp.where(diag, tots, 0.0), axis=0, keepdims=True)
        return e, jnp.concatenate([row0, row1], axis=0)

    def attend(bs, send=True):
        s, e = {}, {}
        for i in range(-AHEAD, len(bs) + BEHIND):
            if i + AHEAD < len(bs):
                s[i + AHEAD] = scores_of(bs[i + AHEAD])
            if 0 <= i < len(bs):
                e[i], stat[bs[i]] = softmax_of(s.pop(i))
            if i >= BEHIND:
                b = bs[i - BEHIND]
                acc[b] = jnp.dot(e.pop(i - BEHIND), vbuf[b], preferred_element_type=f32).astype(bf16)
        for b in bs if send else ():
            x_acc.copy(b).start()
            x_stat.copy(b).start()

    for i in range(1, -(-B // FLIPPED)):
        keys_wait(i)
    pltpu.make_async_copy(values, vbuf, vsem).wait()
    attend([me], send=False)
    x_near.wait_all()
    attend(near_peers)
    x_far.wait_all()
    for i in range(0, len(far_peers), UNROLL):
        attend(far_peers[i : i + UNROLL])
    gacc[me] = acc[me]
    gstat[me] = stat[me]
    for c in later:
        c.wait()
    lam = jnp.broadcast_to(lam_v[...], (heads, heads))
    lam = jnp.sum(
        jnp.where(
            lax.broadcasted_iota(jnp.int32, (heads, heads), 0)
            == lax.broadcasted_iota(jnp.int32, (heads, heads), 1),
            lam,
            0.0,
        ),
        axis=1,
        keepdims=True,
    )
    x_stat.wait_all()
    tops = [gstat[k][0:1] for k in range(n)]
    peak = tops[0]
    for t in tops[1:]:
        peak = jnp.maximum(peak, t)
    facs = [jnp.exp(t - peak) for t in tops]
    total = facs[0] * gstat[0][1:2]
    for k in range(1, n):
        total = total + facs[k] * gstat[k][1:2]
    table = jnp.transpose(
        jnp.concatenate(facs + [jnp.broadcast_to(total, (8, 128))], axis=0)
    )
    x_acc.wait_all()
    merged = table[:lines, 0:1] * gacc[0].astype(f32)
    for k in range(1, n):
        merged = merged + table[:lines, k : k + 1] * gacc[k].astype(f32)
    ratio = merged / table[:lines, n : n + 1]
    normed = []
    for g in range(kv_heads):
        base = g * 2 * half
        head = ratio[base : base + half] - lam[g * half : (g + 1) * half] * ratio[base + half : base + 2 * half]
        mean_sq = jnp.mean(head * head, axis=1, keepdims=True)
        normed.append(head * lax.rsqrt(mean_sq + 1.0 / ctx_total) * hg_v[...])
    mine_n[...] = jnp.concatenate(normed, axis=0).astype(bf16)
    x_n = ex("kv", 7, lambda p: mine_n, all_n)
    x_n.start_all()
    all_n[me] = mine_n[...]
    x_n.wait_all()

    for b in range(B):
        norm_f[b * heads : (b + 1) * heads, :] = all_n[b].astype(f32)
    normed = jnp.concatenate(
        [norm_f[pl.ds(h, B, stride=heads), :].astype(bf16) for h in range(heads)], axis=1
    )
    attn_out = jnp.dot(normed, wo_v[...], preferred_element_type=f32)
    res_v[...] = (tok_v[...].astype(f32) + attn_out).astype(bf16)
    my_y, my_c = my_tp // 2, lax.rem(my_tp, 2)
    res_sent = sems.at[9, 0]

    def res_copy(dy, dc):
        peer = lax.rem(my_y + dy, ny) * 2 + lax.rem(my_c + dc, 2)
        return remote(res_v, all_res.at[my_tp], res_sent, res_sem.at[(ny - dy) % ny], "tp", peer)

    for dy, dc in [(0, 1)] + [(d, c) for d in range(ny - 1, 0, -1) for c in range(2)]:
        res_copy(dy, dc).start()
    all_res[my_tp] = res_v[...]

    cw = up_v.shape[2]
    square = lax.broadcasted_iota(jnp.int32, (R, 128), 0) == lax.broadcasted_iota(
        jnp.int32, (R, 128), 1
    )
    chips = [lax.rem(my_y + dy, ny) for dy in range(ny)]
    ats = [rows_of(y * R, R) for y in chips]
    x_sq, x_up, x_act = [], [], []
    for dy, at in enumerate(ats):
        x_sq.append(
            Exchange(
                "kv",
                kv_peers,
                me,
                lambda p, dy=dy: sq_v.at[dy],
                lambda p, dy=dy: got_sq.at[dy, p],
                got_sq.at[dy, pl.ds(0, n - 1)],
                sems.at[11 + 3 * dy],
            )
        )
        for xs, src_of, dst, i in (
            (x_up, lambda p, at=at: up_v.at[p, at], got_up, 12 + 3 * dy),
            (x_act, lambda p, at=at: mine_act.at[at], all_act, 13 + 3 * dy),
        ):
            xs.append(
                Exchange(
                    "kv",
                    kv_peers,
                    me,
                    src_of,
                    lambda p, dst=dst, at=at: dst.at[p, at],
                    dst.at[pl.ds(0, n - 1), at],
                    sems.at[i],
                )
            )

    for dy, (y, at) in enumerate(zip(chips, ats)):
        arrived = all_res.at[pl.ds(0, 2 if dy else 1)]
        remote(arrived, arrived, res_sent, res_sem.at[dy], "tp", tp_peers[0]).wait_recv()
        every = all_res[pl.ds(y * 2, 2)].reshape(R, cols).astype(f32)
        gained = (every * mg_v[...]).astype(bf16)
        row_sq = jnp.sum(every * every, axis=1, keepdims=True)
        sq_v[dy] = jnp.sum(jnp.where(square, row_sq, 0.0), axis=0, keepdims=True)
        up = jnp.dot(gained, wu_v[...], preferred_element_type=f32)
        for p in range(n):
            up_v[p, at] = up[:, p * cw : (p + 1) * cw].astype(bf16)
        for peer in kv_peers:
            x_sq[dy].copy(peer).start()
            x_up[dy].copy(peer).start()
        got_sq[dy, me] = sq_v[dy]
        got_up[me, at] = up_v[me, at]
    for dy, at in enumerate(ats):
        x_sq[dy].wait_all()
        total = got_sq[dy, 0]
        for k in range(1, n):
            total = total + got_sq[dy, k]
        inv_row = lax.rsqrt(total / full_width + norm_eps)
        inv_two = jnp.sum(jnp.where(square, inv_row, 0.0), axis=1, keepdims=True)
        x_up[dy].wait_all()
        total = got_up[0, at].astype(f32)
        for k in range(1, n):
            total = total + got_up[k, at].astype(f32)
        pre = jnp.maximum(total * inv_two, 0.0)
        mine_act[at, :] = (pre * pre).astype(bf16)
        x_act[dy].start_all()
        all_act[me, at] = mine_act[at, :]

    x_down = ex("tp", 10, lambda p: down_v.at[rows_of(p * B, B)], got_down)
    for dy, (y, at) in enumerate(zip(chips, ats)):
        x_act[dy].wait_all()
        act = jnp.concatenate([all_act[k, at] for k in range(n)], axis=1)
        down_v[at, :] = jnp.dot(act, wd_v[...], preferred_element_type=f32).astype(bf16)
        for peer in [y * 2, y * 2 + 1] if dy else [y * 2 + 1 - my_c]:
            x_down.copy(peer).start()
    got_down[my_tp] = down_v[rows_of(my_tp * B, B), :]
    x_down.wait_all()
    total = got_down[0].astype(f32)
    for k in range(1, n_tp):
        total = total + got_down[k].astype(f32)
    mixed[...] = (res_v[...].astype(f32) + total).astype(bf16)

    x_kv2.wait_all()
    sent = all_res.at[pl.ds(0, n_tp - 1)]
    remote(sent, sent, res_sent, res_sem.at[0], "tp", tp_peers[0]).wait_send()
    once = [x_s, x_q, x_kv, x_far, x_near, x_kv2, x_acc, x_stat, x_n, x_down]
    for x in once + x_sq + x_up + x_act:
        x.drain()


def result_kernel(mixed, kv_out, out, new_keys, new_values, sems):
    copies = [
        pltpu.make_async_copy(src, dst, sems.at[i])
        for i, (src, dst) in enumerate(
            ((mixed, out), (kv_out.at[:, 0], new_keys), (kv_out.at[:, 1], new_values))
        )
    ]
    for c in copies:
        c.start()
    for c in copies:
        c.wait()


def shards(
    tokens,
    cache_keys,
    cache_values,
    attn_gain,
    w_query,
    w_key,
    w_value,
    lambdas,
    head_gain,
    w_out,
    mlp_gain,
    w_up,
    w_down,
):
    B, tok_width = tokens.shape
    n = lax.axis_size("kv")
    n_tp = lax.axis_size("tp")
    kv_heads = cache_keys.shape[2]
    comp = cache_keys.shape[3] // 2
    vd = cache_values.shape[3]
    ctx = cache_keys.shape[1]
    heads = lambdas.shape[0]
    span = ctx * kv_heads
    all_rows = B * n_tp
    hidden = w_up.shape[1]
    cw = hidden // n
    lines = 2 * heads
    assert B == n and comp * 2 == 128 and vd == 128
    V = pltpu.VMEM
    scratch = [
        V(tokens.shape, bf16),
        V((1, tok_width), f32),
        V(w_query.shape, bf16),
        V(w_key.shape, bf16),
        V(w_value.shape, bf16),
        V((1, heads), f32),
        V((1, vd), f32),
        V((1, tok_width), f32),
        V((B, span, 128), bf16),
        V((B, span, 128), bf16),
        V(w_out.shape, bf16),
        V(w_up.shape, bf16),
        V(w_down.shape, bf16),
        DMA((11,)),
        DMA((-(-B // FLIPPED),)),
        DMA,
        V((B * heads, 128), f32),
        V((B, 1, 128), f32),
        V((B * 8, 128), f32),
        V((n, heads, 128), f32),
        V((n, 1, 128), f32),
        V((n, 8, 128), f32),
        V((heads, 128), bf16),
        V((2, kv_heads, 128), bf16),
        V((n, heads, 128), bf16),
        V((n, lines, vd), bf16),
        V((n, 2, 128), f32),
        V((n, lines, vd), bf16),
        V((n, 2, 128), f32),
        V((heads, vd), bf16),
        V((n, heads, vd), bf16),
        V((B * heads, vd), f32),
        V((B, tok_width), bf16),
        V((n_tp, B, tok_width), bf16),
        V((n_tp // 2, 1, 128), f32),
        V((n_tp // 2, n, 1, 128), f32),
        V((n, all_rows, cw), bf16),
        V((n, all_rows, cw), bf16),
        V((all_rows, cw), bf16),
        V((n, all_rows, cw), bf16),
        V((all_rows, tok_width), bf16),
        V((n_tp, B, tok_width), bf16),
        DMA((11 + 3 * (n_tp // 2), 2)),
        DMA((n_tp // 2,)),
        V((FLIPPED, 128, span), bf16),
    ]
    mixed, kv_out = pl.pallas_call(
        functools.partial(
            layer_kernel, n, n_tp, kv_heads, tok_width * n, ctx * n, comp ** (-0.5)
        ),
        out_shape=(
            jax.ShapeDtypeStruct((B, tok_width), bf16),
            jax.ShapeDtypeStruct((n, 2, kv_heads, 128), bf16),
        ),
        in_specs=[HBM] * 13,
        out_specs=(VM, VM),
        scratch_shapes=scratch,
        compiler_params=pltpu.CompilerParams(
            collective_id=0, has_side_effects=True, vmem_limit_bytes=48 * 1024 * 1024
        ),
    )(
        *[
            pltpu.with_memory_space_constraint(x, pltpu.HBM)
            for x in (
                tokens,
                cache_keys.reshape(B, span, 128),
                cache_values.reshape(B, span, vd),
                attn_gain.reshape(1, tok_width),
                w_query,
                w_key,
                w_value,
                lambdas.reshape(1, heads),
                head_gain.reshape(1, vd),
                w_out,
                mlp_gain.reshape(1, tok_width),
                w_up,
                w_down,
            )
        ]
    )
    return pl.pallas_call(
        result_kernel,
        out_shape=(
            jax.ShapeDtypeStruct(mixed.shape, bf16),
            jax.ShapeDtypeStruct((n, kv_heads, 128), bf16),
            jax.ShapeDtypeStruct((n, kv_heads, 128), bf16),
        ),
        in_specs=[VM, VM],
        out_specs=(HBM, HBM, HBM),
        scratch_shapes=[DMA((3,))],
        compiler_params=pltpu.CompilerParams(vmem_limit_bytes=1024 * 1024),
    )(mixed, kv_out)


def solution(mesh):
    in_specs = (
        P("tp", "kv"),
        P("tp", "kv", None, None),
        P("tp", "kv", None, None),
        P("kv"),
        P("kv", None),
        P("kv", None),
        P("kv", None),
        P(),
        P(),
        P(None, "kv"),
        P("kv"),
        P("kv", "tp"),
        P("tp", "kv"),
    )
    out_specs = (P("tp", "kv"), P("tp", None, None), P("tp", None, None))
    return jax.shard_map(shards, mesh=mesh, in_specs=in_specs, out_specs=out_specs, check_vma=False)
```

```python
import functools

import jax
import jax.numpy as jnp
from jax import lax
from jax.experimental import pallas as pl
from jax.experimental.pallas import tpu as pltpu
from jax.sharding import PartitionSpec as P

norm_eps = 1e-06
f32 = jnp.float32
bf16 = jnp.bfloat16
VM = pl.BlockSpec(memory_space=pltpu.VMEM)
HBM = pl.BlockSpec(memory_space=pltpu.HBM)
DMA = pltpu.SemaphoreType.DMA
NT = (((1,), (1,)), ((), ()))
UNROLL = 4
AHEAD = 2
FLIPPED = 11
BEHIND = 1


def remote(src, dst, send, recv, axis, peer):
    return pltpu.make_async_remote_copy(
        src_ref=src,
        dst_ref=dst,
        send_sem=send,
        recv_sem=recv,
        device_id={axis: peer},
        device_id_type=pl.DeviceIdType.MESH,
    )


class Exchange:
    def __init__(self, axis, peers, me, src_of, dst_of, all_dst, sems):
        self.axis, self.peers, self.me = axis, peers, me
        self.src_of, self.dst_of, self.all_dst = src_of, dst_of, all_dst
        self.send, self.recv = sems

    def copy(self, peer):
        return remote(
            self.src_of(peer), self.dst_of(self.me), self.send, self.recv, self.axis, peer
        )

    def start_all(self):
        for peer in self.peers:
            self.copy(peer).start()

    def everything(self):
        return remote(self.all_dst, self.all_dst, self.send, self.recv, self.axis, self.peers[0])

    def wait_all(self):
        self.everything().wait_recv()

    def drain(self):
        self.everything().wait_send()


def offsets(outer, inner, wrap_inner):
    def far(d, size, wrap):
        return min(d, size - d) if wrap else d % 2

    every = [(a, b) for a in range(outer) for b in range(inner)]
    every.sort(key=lambda o: -(far(o[0], outer, True) + far(o[1], inner, wrap_inner) / 1.5))
    return every


def rows_of(start, size):
    return pl.ds(pl.multiple_of(start, size), size)


def layer_kernel(
    n,
    n_tp,
    kv_heads,
    full_width,
    ctx_total,
    scale,
    tokens,
    keys,
    values,
    attn_gain,
    w_query,
    w_key,
    w_value,
    lambdas,
    head_gain,
    w_out,
    mlp_gain,
    w_up,
    w_down,
    mixed,
    kv_out,
    tok_v,
    ag_v,
    wq_v,
    wk_v,
    wv_v,
    lam_v,
    hg_v,
    mg_v,
    kbuf,
    vbuf,
    wo_v,
    wu_v,
    wd_v,
    lsem,
    ksem,
    vsem,
    part_q,
    part_s,
    part_kv,
    got_q,
    got_s,
    got_kv,
    mine_q,
    mine_kv,
    all_q,
    acc,
    stat,
    gacc,
    gstat,
    mine_n,
    all_n,
    norm_f,
    res_v,
    all_res,
    sq_v,
    got_sq,
    up_v,
    got_up,
    mine_act,
    all_act,
    down_v,
    got_down,
    sems,
    res_sem,
    sent,
    flipped,
):
    me = lax.axis_index("kv")
    my_tp = lax.axis_index("tp")
    B = tokens.shape[0]
    heads = got_q.shape[1]
    half = heads // kv_heads
    lines = 2 * heads
    span = keys.shape[1]
    cols = tok_v.shape[1]
    all_rows = B * n_tp
    R = 2 * B
    groups = span // 128

    def order(at, outer, inner, wrap_inner):
        a, b = at // inner, lax.rem(at, inner)
        return [
            lax.rem(a + da, outer) * inner + lax.rem(b + db, inner)
            for da, db in offsets(outer, inner, wrap_inner)
        ]

    side = int(n**0.5)
    ny = n_tp // 2
    kv_order = order(me, side, side, True)
    kv_peers = kv_order[:-1]
    near_peers, far_peers = kv_order[-5:-1], kv_order[:-5]
    tp_peers = order(my_tp, ny, 2, False)[:-1]

    def ex(axis, i, src_of, dst, peers=None):
        every, at = (kv_peers, me) if axis == "kv" else (tp_peers, my_tp)
        peers = every if peers is None else peers
        return Exchange(
            axis, peers, at, src_of, lambda p: dst.at[p], dst.at[pl.ds(0, len(peers))], (sent, sems.at[i])
        )

    first = [(tokens, tok_v), (attn_gain, ag_v), (w_query, wq_v), (w_key, wk_v), (w_value, wv_v)]
    later = [
        (lambdas, lam_v),
        (head_gain, hg_v),
        (w_out, wo_v),
        (mlp_gain, mg_v),
        (w_up, wu_v),
        (w_down, wd_v),
    ]
    first = [pltpu.make_async_copy(a, b, lsem.at[i]) for i, (a, b) in enumerate(first)]
    later = [pltpu.make_async_copy(a, b, lsem.at[len(first) + i]) for i, (a, b) in enumerate(later)]
    for c in first:
        c.start()
    barrier = pltpu.get_barrier_semaphore()
    for axis, peers in (("kv", kv_peers), ("tp", tp_peers)):
        for peer in peers:
            pl.semaphore_signal(
                barrier, inc=1, device_id={axis: peer}, device_id_type=pl.DeviceIdType.MESH
            )
    for i, b in enumerate(kv_order):
        pltpu.make_async_copy(keys.at[b], kbuf.at[b], ksem.at[i // FLIPPED]).start()
    for b in kv_order:
        pltpu.make_async_copy(values.at[b], vbuf.at[b], vsem).start()

    for c in first:
        c.wait()

    def keys_wait(i):
        first, size = i * FLIPPED, min(FLIPPED, B - i * FLIPPED)
        at = pl.ds(first, size)
        pltpu.make_async_copy(keys.at[at], kbuf.at[at], ksem.at[i]).wait()

    eye = jnp.where(
        lax.broadcasted_iota(jnp.int32, (128, 128), 0)
        == lax.broadcasted_iota(jnp.int32, (128, 128), 1),
        1.0,
        0.0,
    ).astype(bf16)

    def flip():
        keys_wait(0)
        for i in range(FLIPPED):
            flipped[i] = lax.dot_general(
                eye, kbuf[kv_order[i]], NT, preferred_element_type=f32
            ).astype(bf16)

    for c in later:
        c.start()

    tok_f = tok_v[...].astype(f32)
    scaled = (tok_f * ag_v[...]).astype(bf16)
    squares = jnp.broadcast_to(jnp.sum(tok_f * tok_f, axis=1, keepdims=True), (B, 128))
    for r in range(B):
        part_s[r] = squares[r : r + 1]
    product = jnp.dot(scaled, wq_v[...], preferred_element_type=f32)
    for h in range(heads):
        part_q[pl.ds(h, B, stride=heads), :] = product[:, h * 128 : (h + 1) * 128]
    pieces = 0
    for w in (wk_v, wv_v):
        product = jnp.dot(scaled, w[...], preferred_element_type=f32)
        for h in range(product.shape[1] // 128):
            part_kv[pl.ds(pieces, B, stride=8), :] = product[:, h * 128 : (h + 1) * 128]
            pieces += 1
    for h in range(pieces, 8):
        part_kv[pl.ds(h, B, stride=8), :] = jnp.zeros((B, 128), f32)

    x_q = ex("kv", 0, lambda p: part_q.at[rows_of(p * heads, heads)], got_q)
    x_s = ex("kv", 1, lambda p: part_s.at[p], got_s)
    x_kv = ex("kv", 2, lambda p: part_kv.at[rows_of(p * 8, 8)], got_kv)
    pl.semaphore_wait(barrier, n - 1 + n_tp - 1)
    for peer in kv_peers:
        x_s.copy(peer).start()
        x_q.copy(peer).start()
    x_kv.start_all()
    got_q[me] = part_q[rows_of(me * heads, heads), :]
    got_s[me] = part_s[me]
    got_kv[me] = part_kv[rows_of(me * 8, 8), :]
    flip()
    x_s.wait_all()
    total = got_s[0]
    for k in range(1, n):
        total = total + got_s[k]
    inv_one = lax.rsqrt(total / full_width + norm_eps)
    x_q.wait_all()
    total = got_q[0]
    for k in range(1, n):
        total = total + got_q[k]
    query = (total * inv_one).astype(bf16).astype(f32) * scale
    mine_q[...] = query.astype(bf16)
    x_far = ex("kv", 3, lambda p: mine_q, all_q, far_peers)
    x_near = ex("kv", 8, lambda p: mine_q, all_q, near_peers)
    x_far.start_all()
    x_near.start_all()
    all_q[me] = mine_q[...]
    x_kv.wait_all()
    total = got_kv[0]
    for k in range(1, n):
        total = total + got_kv[k]
    new_kv = (total * inv_one).astype(bf16)
    for i in range(2):
        mine_kv[i] = new_kv[i * kv_heads : (i + 1) * kv_heads]
    x_kv2 = ex("kv", 4, lambda p: mine_kv, kv_out)
    x_kv2.start_all()
    kv_out[me] = mine_kv[...]

    lane = lax.broadcasted_iota(jnp.int32, (heads, 128), 1)
    even = lax.rem(lane, 2) == 0
    low = lane < 64
    diag = lax.broadcasted_iota(jnp.int32, (lines, 128), 1) == lax.broadcasted_iota(
        jnp.int32, (lines, 128), 0
    )

    x_acc = ex("kv", 5, lambda p: acc.at[p], gacc)
    x_stat = ex("kv", 6, lambda p: stat.at[p], gstat)

    def scores_of(b):
        q = all_q[b].astype(f32)
        lo = jnp.where(low, q, 0.0)
        hi = jnp.where(low, 0.0, q)
        q_lines = jnp.concatenate([lo[:half], hi[:half], lo[half:], hi[half:]], axis=0).astype(bf16)
        for i in range(FLIPPED):
            if b is kv_order[i]:
                return jnp.dot(q_lines, flipped[i], preferred_element_type=f32)
        return lax.dot_general(q_lines, kbuf[b], NT, preferred_element_type=f32)

    def softmax_of(s):
        m = [
            jnp.where(even, s[:heads, c * 128 : (c + 1) * 128], s[heads:, c * 128 : (c + 1) * 128])
            for c in range(groups)
        ]
        top = m[0]
        for c in range(1, groups):
            top = jnp.maximum(top, m[c])
        top0 = jnp.max(jnp.where(even, top, -jnp.inf), axis=1, keepdims=True)
        top1 = jnp.max(jnp.where(even, -jnp.inf, top), axis=1, keepdims=True)
        top = jnp.where(even, top0, top1)
        m = [jnp.exp(x - top) for x in m]
        total = m[0]
        for c in range(1, groups):
            total = total + m[c]
        tot0 = jnp.sum(jnp.where(even, total, 0.0), axis=1, keepdims=True)
        tot1 = jnp.sum(jnp.where(even, 0.0, total), axis=1, keepdims=True)
        e = jnp.concatenate(
            [
                jnp.concatenate([jnp.where(even, x, 0.0).astype(bf16) for x in m], axis=1),
                jnp.concatenate([jnp.where(even, 0.0, x).astype(bf16) for x in m], axis=1),
            ],
            axis=0,
        )
        tops = jnp.concatenate([top0, top1], axis=0)
        tots = jnp.concatenate([tot0, tot1], axis=0)
        row0 = jnp.sum(jnp.where(diag, tops, 0.0), axis=0, keepdims=True)
        row1 = jnp.sum(jnp.where(diag, tots, 0.0), axis=0, keepdims=True)
        return e, jnp.concatenate([row0, row1], axis=0)

    def attend(bs, send=True):
        s, e = {}, {}
        for i in range(-AHEAD, len(bs) + BEHIND):
            if i + AHEAD < len(bs):
                s[i + AHEAD] = scores_of(bs[i + AHEAD])
            if 0 <= i < len(bs):
                e[i], stat[bs[i]] = softmax_of(s.pop(i))
            if i >= BEHIND:
                b = bs[i - BEHIND]
                acc[b] = jnp.dot(e.pop(i - BEHIND), vbuf[b], preferred_element_type=f32).astype(bf16)
        for b in bs if send else ():
            x_acc.copy(b).start()
            x_stat.copy(b).start()

    for i in range(1, -(-B // FLIPPED)):
        keys_wait(i)
    pltpu.make_async_copy(values, vbuf, vsem).wait()
    attend([me], send=False)
    x_near.wait_all()
    attend(near_peers)
    x_far.wait_all()
    for i in range(0, len(far_peers), UNROLL):
        attend(far_peers[i : i + UNROLL])
    gacc[me] = acc[me]
    gstat[me] = stat[me]
    for c in later:
        c.wait()
    lam = jnp.broadcast_to(lam_v[...], (heads, heads))
    lam = jnp.sum(
        jnp.where(
            lax.broadcasted_iota(jnp.int32, (heads, heads), 0)
            == lax.broadcasted_iota(jnp.int32, (heads, heads), 1),
            lam,
            0.0,
        ),
        axis=1,
        keepdims=True,
    )
    x_stat.wait_all()
    tops = [gstat[k][0:1] for k in range(n)]
    peak = tops[0]
    for t in tops[1:]:
        peak = jnp.maximum(peak, t)
    facs = [jnp.exp(t - peak) for t in tops]
    total = facs[0] * gstat[0][1:2]
    for k in range(1, n):
        total = total + facs[k] * gstat[k][1:2]
    table = jnp.transpose(
        jnp.concatenate(facs + [jnp.broadcast_to(total, (8, 128))], axis=0)
    )
    x_acc.wait_all()
    merged = table[:lines, 0:1] * gacc[0].astype(f32)
    for k in range(1, n):
        merged = merged + table[:lines, k : k + 1] * gacc[k].astype(f32)
    ratio = merged / table[:lines, n : n + 1]
    normed = []
    for g in range(kv_heads):
        base = g * 2 * half
        head = ratio[base : base + half] - lam[g * half : (g + 1) * half] * ratio[base + half : base + 2 * half]
        mean_sq = jnp.mean(head * head, axis=1, keepdims=True)
        normed.append(head * lax.rsqrt(mean_sq + 1.0 / ctx_total) * hg_v[...])
    mine_n[...] = jnp.concatenate(normed, axis=0).astype(bf16)
    x_n = ex("kv", 7, lambda p: mine_n, all_n)
    x_n.start_all()
    all_n[me] = mine_n[...]
    x_n.wait_all()

    for b in range(B):
        norm_f[b * heads : (b + 1) * heads, :] = all_n[b].astype(f32)
    normed = jnp.concatenate(
        [norm_f[pl.ds(h, B, stride=heads), :].astype(bf16) for h in range(heads)], axis=1
    )
    attn_out = jnp.dot(normed, wo_v[...], preferred_element_type=f32)
    res_v[...] = (tok_v[...].astype(f32) + attn_out).astype(bf16)
    my_y, my_c = my_tp // 2, lax.rem(my_tp, 2)
    res_sent = sent

    def res_copy(dy, dc):
        peer = lax.rem(my_y + dy, ny) * 2 + lax.rem(my_c + dc, 2)
        return remote(res_v, all_res.at[my_tp], res_sent, res_sem.at[(ny - dy) % ny], "tp", peer)

    for dy, dc in [(0, 1)] + [(d, c) for d in range(ny - 1, 0, -1) for c in range(2)]:
        res_copy(dy, dc).start()
    all_res[my_tp] = res_v[...]

    cw = up_v.shape[2]
    square = lax.broadcasted_iota(jnp.int32, (R, 128), 0) == lax.broadcasted_iota(
        jnp.int32, (R, 128), 1
    )
    chips = [lax.rem(my_y + dy, ny) for dy in range(ny)]
    ats = [rows_of(y * R, R) for y in chips]
    x_sq, x_up, x_act = [], [], []
    for dy, at in enumerate(ats):
        x_sq.append(
            Exchange(
                "kv",
                kv_peers,
                me,
                lambda p, dy=dy: sq_v.at[dy],
                lambda p, dy=dy: got_sq.at[dy, p],
                got_sq.at[dy, pl.ds(0, n - 1)],
                (sent, sems.at[11 + 3 * dy]),
            )
        )
        for xs, src_of, dst, i in (
            (x_up, lambda p, at=at: up_v.at[p, at], got_up, 12 + 3 * dy),
            (x_act, lambda p, at=at: mine_act.at[at], all_act, 13 + 3 * dy),
        ):
            xs.append(
                Exchange(
                    "kv",
                    kv_peers,
                    me,
                    src_of,
                    lambda p, dst=dst, at=at: dst.at[p, at],
                    dst.at[pl.ds(0, n - 1), at],
                    (sent, sems.at[i]),
                )
            )

    for dy, (y, at) in enumerate(zip(chips, ats)):
        arrived = all_res.at[pl.ds(0, 2 if dy else 1)]
        remote(arrived, arrived, res_sent, res_sem.at[dy], "tp", tp_peers[0]).wait_recv()
        every = all_res[pl.ds(y * 2, 2)].reshape(R, cols).astype(f32)
        gained = (every * mg_v[...]).astype(bf16)
        row_sq = jnp.sum(every * every, axis=1, keepdims=True)
        sq_v[dy] = jnp.sum(jnp.where(square, row_sq, 0.0), axis=0, keepdims=True)
        up = jnp.dot(gained, wu_v[...], preferred_element_type=f32)
        for p in range(n):
            up_v[p, at] = up[:, p * cw : (p + 1) * cw].astype(bf16)
        for peer in kv_peers:
            x_sq[dy].copy(peer).start()
            x_up[dy].copy(peer).start()
        got_sq[dy, me] = sq_v[dy]
        got_up[me, at] = up_v[me, at]
    for dy, at in enumerate(ats):
        x_sq[dy].wait_all()
        total = got_sq[dy, 0]
        for k in range(1, n):
            total = total + got_sq[dy, k]
        inv_row = lax.rsqrt(total / full_width + norm_eps)
        inv_two = jnp.sum(jnp.where(square, inv_row, 0.0), axis=1, keepdims=True)
        x_up[dy].wait_all()
        total = got_up[0, at].astype(f32)
        for k in range(1, n):
            total = total + got_up[k, at].astype(f32)
        pre = jnp.maximum(total * inv_two, 0.0)
        mine_act[at, :] = (pre * pre).astype(bf16)
        x_act[dy].start_all()
        all_act[me, at] = mine_act[at, :]

    x_down = ex("tp", 10, lambda p: down_v.at[rows_of(p * B, B)], got_down)
    for dy, (y, at) in enumerate(zip(chips, ats)):
        x_act[dy].wait_all()
        act = jnp.concatenate([all_act[k, at] for k in range(n)], axis=1)
        down_v[at, :] = jnp.dot(act, wd_v[...], preferred_element_type=f32).astype(bf16)
        for peer in [y * 2, y * 2 + 1] if dy else [y * 2 + 1 - my_c]:
            x_down.copy(peer).start()
    got_down[my_tp] = down_v[rows_of(my_tp * B, B), :]
    x_down.wait_all()
    total = got_down[0].astype(f32)
    for k in range(1, n_tp):
        total = total + got_down[k].astype(f32)
    mixed[...] = (res_v[...].astype(f32) + total).astype(bf16)

    x_kv2.wait_all()
    sent = all_res.at[pl.ds(0, n_tp - 1)]
    remote(sent, sent, res_sent, res_sem.at[0], "tp", tp_peers[0]).wait_send()
    once = [x_s, x_q, x_kv, x_far, x_near, x_kv2, x_acc, x_stat, x_n, x_down]
    for x in once + x_sq + x_up + x_act:
        x.drain()


def result_kernel(mixed, kv_out, out, new_keys, new_values, sems):
    copies = [
        pltpu.make_async_copy(src, dst, sems.at[i])
        for i, (src, dst) in enumerate(
            ((mixed, out), (kv_out.at[:, 0], new_keys), (kv_out.at[:, 1], new_values))
        )
    ]
    for c in copies:
        c.start()
    for c in copies:
        c.wait()


def shards(
    tokens,
    cache_keys,
    cache_values,
    attn_gain,
    w_query,
    w_key,
    w_value,
    lambdas,
    head_gain,
    w_out,
    mlp_gain,
    w_up,
    w_down,
):
    B, tok_width = tokens.shape
    n = lax.axis_size("kv")
    n_tp = lax.axis_size("tp")
    kv_heads = cache_keys.shape[2]
    comp = cache_keys.shape[3] // 2
    vd = cache_values.shape[3]
    ctx = cache_keys.shape[1]
    heads = lambdas.shape[0]
    span = ctx * kv_heads
    all_rows = B * n_tp
    hidden = w_up.shape[1]
    cw = hidden // n
    lines = 2 * heads
    assert B == n and comp * 2 == 128 and vd == 128
    V = pltpu.VMEM
    scratch = [
        V(tokens.shape, bf16),
        V((1, tok_width), f32),
        V(w_query.shape, bf16),
        V(w_key.shape, bf16),
        V(w_value.shape, bf16),
        V((1, heads), f32),
        V((1, vd), f32),
        V((1, tok_width), f32),
        V((B, span, 128), bf16),
        V((B, span, 128), bf16),
        V(w_out.shape, bf16),
        V(w_up.shape, bf16),
        V(w_down.shape, bf16),
        DMA((11,)),
        DMA((-(-B // FLIPPED),)),
        DMA,
        V((B * heads, 128), f32),
        V((B, 1, 128), f32),
        V((B * 8, 128), f32),
        V((n, heads, 128), f32),
        V((n, 1, 128), f32),
        V((n, 8, 128), f32),
        V((heads, 128), bf16),
        V((2, kv_heads, 128), bf16),
        V((n, heads, 128), bf16),
        V((n, lines, vd), bf16),
        V((n, 2, 128), f32),
        V((n, lines, vd), bf16),
        V((n, 2, 128), f32),
        V((heads, vd), bf16),
        V((n, heads, vd), bf16),
        V((B * heads, vd), f32),
        V((B, tok_width), bf16),
        V((n_tp, B, tok_width), bf16),
        V((n_tp // 2, 1, 128), f32),
        V((n_tp // 2, n, 1, 128), f32),
        V((n, all_rows, cw), bf16),
        V((n, all_rows, cw), bf16),
        V((all_rows, cw), bf16),
        V((n, all_rows, cw), bf16),
        V((all_rows, tok_width), bf16),
        V((n_tp, B, tok_width), bf16),
        DMA((11 + 3 * (n_tp // 2),)),
        DMA((n_tp // 2,)),
        DMA,
        V((FLIPPED, 128, span), bf16),
    ]
    mixed, kv_out = pl.pallas_call(
        functools.partial(
            layer_kernel, n, n_tp, kv_heads, tok_width * n, ctx * n, comp ** (-0.5)
        ),
        out_shape=(
            jax.ShapeDtypeStruct((B, tok_width), bf16),
            jax.ShapeDtypeStruct((n, 2, kv_heads, 128), bf16),
        ),
        in_specs=[HBM] * 13,
        out_specs=(VM, VM),
        scratch_shapes=scratch,
        compiler_params=pltpu.CompilerParams(
            collective_id=0, has_side_effects=True, vmem_limit_bytes=48 * 1024 * 1024
        ),
    )(
        *[
            pltpu.with_memory_space_constraint(x, pltpu.HBM)
            for x in (
                tokens,
                cache_keys.reshape(B, span, 128),
                cache_values.reshape(B, span, vd),
                attn_gain.reshape(1, tok_width),
                w_query,
                w_key,
                w_value,
                lambdas.reshape(1, heads),
                head_gain.reshape(1, vd),
                w_out,
                mlp_gain.reshape(1, tok_width),
                w_up,
                w_down,
            )
        ]
    )
    return pl.pallas_call(
        result_kernel,
        out_shape=(
            jax.ShapeDtypeStruct(mixed.shape, bf16),
            jax.ShapeDtypeStruct((n, kv_heads, 128), bf16),
            jax.ShapeDtypeStruct((n, kv_heads, 128), bf16),
        ),
        in_specs=[VM, VM],
        out_specs=(HBM, HBM, HBM),
        scratch_shapes=[DMA((3,))],
        compiler_params=pltpu.CompilerParams(vmem_limit_bytes=1024 * 1024),
    )(mixed, kv_out)


def solution(mesh):
    in_specs = (
        P("tp", "kv"),
        P("tp", "kv", None, None),
        P("tp", "kv", None, None),
        P("kv"),
        P("kv", None),
        P("kv", None),
        P("kv", None),
        P(),
        P(),
        P(None, "kv"),
        P("kv"),
        P("kv", "tp"),
        P("tp", "kv"),
    )
    out_specs = (P("tp", "kv"), P("tp", None, None), P("tp", None, None))
    return jax.shard_map(shards, mesh=mesh, in_specs=in_specs, out_specs=out_specs, check_vma=False)
```

```python
import functools

import jax
import jax.numpy as jnp
from jax import lax
from jax.experimental import pallas as pl
from jax.experimental.pallas import tpu as pltpu
from jax.sharding import PartitionSpec as P

norm_eps = 1e-06
f32 = jnp.float32
bf16 = jnp.bfloat16
VM = pl.BlockSpec(memory_space=pltpu.VMEM)
HBM = pl.BlockSpec(memory_space=pltpu.HBM)
DMA = pltpu.SemaphoreType.DMA
NT = (((1,), (1,)), ((), ()))
UNROLL = 4
AHEAD = 3
FLIPPED = 11
BEHIND = 1


def remote(src, dst, send, recv, axis, peer):
    return pltpu.make_async_remote_copy(
        src_ref=src,
        dst_ref=dst,
        send_sem=send,
        recv_sem=recv,
        device_id={axis: peer},
        device_id_type=pl.DeviceIdType.MESH,
    )


class Exchange:
    def __init__(self, axis, peers, me, src_of, dst_of, all_dst, sems):
        self.axis, self.peers, self.me = axis, peers, me
        self.src_of, self.dst_of, self.all_dst = src_of, dst_of, all_dst
        self.send, self.recv = sems

    def copy(self, peer):
        return remote(
            self.src_of(peer), self.dst_of(self.me), self.send, self.recv, self.axis, peer
        )

    def start_all(self):
        for peer in self.peers:
            self.copy(peer).start()

    def everything(self):
        return remote(self.all_dst, self.all_dst, self.send, self.recv, self.axis, self.peers[0])

    def wait_all(self):
        self.everything().wait_recv()

    def drain(self):
        self.everything().wait_send()


def offsets(outer, inner, wrap_inner):
    def far(d, size, wrap):
        return min(d, size - d) if wrap else d % 2

    every = [(a, b) for a in range(outer) for b in range(inner)]
    every.sort(key=lambda o: -(far(o[0], outer, True) + far(o[1], inner, wrap_inner) / 1.5))
    return every


def rows_of(start, size):
    return pl.ds(pl.multiple_of(start, size), size)


def layer_kernel(
    n,
    n_tp,
    kv_heads,
    full_width,
    ctx_total,
    scale,
    tokens,
    keys,
    values,
    attn_gain,
    w_query,
    w_key,
    w_value,
    lambdas,
    head_gain,
    w_out,
    mlp_gain,
    w_up,
    w_down,
    mixed,
    kv_out,
    tok_v,
    ag_v,
    wq_v,
    wk_v,
    wv_v,
    lam_v,
    hg_v,
    mg_v,
    kbuf,
    vbuf,
    wo_v,
    wu_v,
    wd_v,
    lsem,
    ksem,
    vsem,
    part_q,
    part_s,
    part_kv,
    got_q,
    got_s,
    got_kv,
    mine_q,
    mine_kv,
    all_q,
    acc,
    stat,
    gacc,
    gstat,
    mine_n,
    all_n,
    norm_f,
    res_v,
    all_res,
    sq_v,
    got_sq,
    up_v,
    got_up,
    mine_act,
    all_act,
    down_v,
    got_down,
    sems,
    res_sem,
    sent,
    flipped,
):
    me = lax.axis_index("kv")
    my_tp = lax.axis_index("tp")
    B = tokens.shape[0]
    heads = got_q.shape[1]
    half = heads // kv_heads
    lines = 2 * heads
    span = keys.shape[1]
    cols = tok_v.shape[1]
    all_rows = B * n_tp
    R = 2 * B
    groups = span // 128

    def order(at, outer, inner, wrap_inner):
        a, b = at // inner, lax.rem(at, inner)
        return [
            lax.rem(a + da, outer) * inner + lax.rem(b + db, inner)
            for da, db in offsets(outer, inner, wrap_inner)
        ]

    side = int(n**0.5)
    ny = n_tp // 2
    kv_order = order(me, side, side, True)
    kv_peers = kv_order[:-1]
    near_peers, far_peers = kv_order[-5:-1], kv_order[:-5]
    tp_peers = order(my_tp, ny, 2, False)[:-1]

    def ex(axis, i, src_of, dst, peers=None):
        every, at = (kv_peers, me) if axis == "kv" else (tp_peers, my_tp)
        peers = every if peers is None else peers
        return Exchange(
            axis, peers, at, src_of, lambda p: dst.at[p], dst.at[pl.ds(0, len(peers))], (sent, sems.at[i])
        )

    first = [(tokens, tok_v), (attn_gain, ag_v), (w_query, wq_v), (w_key, wk_v), (w_value, wv_v)]
    later = [
        (lambdas, lam_v),
        (head_gain, hg_v),
        (w_out, wo_v),
        (mlp_gain, mg_v),
        (w_up, wu_v),
        (w_down, wd_v),
    ]
    first = [pltpu.make_async_copy(a, b, lsem.at[i]) for i, (a, b) in enumerate(first)]
    later = [pltpu.make_async_copy(a, b, lsem.at[len(first) + i]) for i, (a, b) in enumerate(later)]
    for c in first:
        c.start()
    barrier = pltpu.get_barrier_semaphore()
    for axis, peers in (("kv", kv_peers), ("tp", tp_peers)):
        for peer in peers:
            pl.semaphore_signal(
                barrier, inc=1, device_id={axis: peer}, device_id_type=pl.DeviceIdType.MESH
            )
    for i, b in enumerate(kv_order):
        pltpu.make_async_copy(keys.at[b], kbuf.at[b], ksem.at[i // FLIPPED]).start()
    for b in kv_order:
        pltpu.make_async_copy(values.at[b], vbuf.at[b], vsem).start()

    for c in first:
        c.wait()

    def keys_wait(i):
        first, size = i * FLIPPED, min(FLIPPED, B - i * FLIPPED)
        at = pl.ds(first, size)
        pltpu.make_async_copy(keys.at[at], kbuf.at[at], ksem.at[i]).wait()

    eye = jnp.where(
        lax.broadcasted_iota(jnp.int32, (128, 128), 0)
        == lax.broadcasted_iota(jnp.int32, (128, 128), 1),
        1.0,
        0.0,
    ).astype(bf16)

    def flip():
        keys_wait(0)
        for i in range(FLIPPED):
            flipped[i] = lax.dot_general(
                eye, kbuf[kv_order[i]], NT, preferred_element_type=f32
            ).astype(bf16)

    for c in later:
        c.start()

    tok_f = tok_v[...].astype(f32)
    scaled = (tok_f * ag_v[...]).astype(bf16)
    squares = jnp.broadcast_to(jnp.sum(tok_f * tok_f, axis=1, keepdims=True), (B, 128))
    for r in range(B):
        part_s[r] = squares[r : r + 1]
    product = jnp.dot(scaled, wq_v[...], preferred_element_type=f32)
    for h in range(heads):
        part_q[pl.ds(h, B, stride=heads), :] = product[:, h * 128 : (h + 1) * 128]
    pieces = 0
    for w in (wk_v, wv_v):
        product = jnp.dot(scaled, w[...], preferred_element_type=f32)
        for h in range(product.shape[1] // 128):
            part_kv[pl.ds(pieces, B, stride=8), :] = product[:, h * 128 : (h + 1) * 128]
            pieces += 1
    for h in range(pieces, 8):
        part_kv[pl.ds(h, B, stride=8), :] = jnp.zeros((B, 128), f32)

    x_q = ex("kv", 0, lambda p: part_q.at[rows_of(p * heads, heads)], got_q)
    x_s = ex("kv", 1, lambda p: part_s.at[p], got_s)
    x_kv = ex("kv", 2, lambda p: part_kv.at[rows_of(p * 8, 8)], got_kv)
    pl.semaphore_wait(barrier, n - 1 + n_tp - 1)
    for peer in kv_peers:
        x_s.copy(peer).start()
        x_q.copy(peer).start()
    x_kv.start_all()
    got_q[me] = part_q[rows_of(me * heads, heads), :]
    got_s[me] = part_s[me]
    got_kv[me] = part_kv[rows_of(me * 8, 8), :]
    flip()
    x_s.wait_all()
    total = got_s[0]
    for k in range(1, n):
        total = total + got_s[k]
    inv_one = lax.rsqrt(total / full_width + norm_eps)
    x_q.wait_all()
    total = got_q[0]
    for k in range(1, n):
        total = total + got_q[k]
    query = (total * inv_one).astype(bf16).astype(f32) * scale
    mine_q[...] = query.astype(bf16)
    x_far = ex("kv", 3, lambda p: mine_q, all_q, far_peers)
    x_near = ex("kv", 8, lambda p: mine_q, all_q, near_peers)
    x_far.start_all()
    x_near.start_all()
    all_q[me] = mine_q[...]
    x_kv.wait_all()
    total = got_kv[0]
    for k in range(1, n):
        total = total + got_kv[k]
    new_kv = (total * inv_one).astype(bf16)
    for i in range(2):
        mine_kv[i] = new_kv[i * kv_heads : (i + 1) * kv_heads]
    x_kv2 = ex("kv", 4, lambda p: mine_kv, kv_out)
    x_kv2.start_all()
    kv_out[me] = mine_kv[...]

    lane = lax.broadcasted_iota(jnp.int32, (heads, 128), 1)
    even = lax.rem(lane, 2) == 0
    low = lane < 64
    diag = lax.broadcasted_iota(jnp.int32, (lines, 128), 1) == lax.broadcasted_iota(
        jnp.int32, (lines, 128), 0
    )

    x_acc = ex("kv", 5, lambda p: acc.at[p], gacc)
    x_stat = ex("kv", 6, lambda p: stat.at[p], gstat)

    def scores_of(b):
        q = all_q[b].astype(f32)
        lo = jnp.where(low, q, 0.0)
        hi = jnp.where(low, 0.0, q)
        q_lines = jnp.concatenate([lo[:half], hi[:half], lo[half:], hi[half:]], axis=0).astype(bf16)
        for i in range(FLIPPED):
            if b is kv_order[i]:
                return jnp.dot(q_lines, flipped[i], preferred_element_type=f32)
        return lax.dot_general(q_lines, kbuf[b], NT, preferred_element_type=f32)

    def softmax_of(s):
        m = [
            jnp.where(even, s[:heads, c * 128 : (c + 1) * 128], s[heads:, c * 128 : (c + 1) * 128])
            for c in range(groups)
        ]
        top = m[0]
        for c in range(1, groups):
            top = jnp.maximum(top, m[c])
        top0 = jnp.max(jnp.where(even, top, -jnp.inf), axis=1, keepdims=True)
        top1 = jnp.max(jnp.where(even, -jnp.inf, top), axis=1, keepdims=True)
        top = jnp.where(even, top0, top1)
        m = [jnp.exp(x - top) for x in m]
        total = m[0]
        for c in range(1, groups):
            total = total + m[c]
        tot0 = jnp.sum(jnp.where(even, total, 0.0), axis=1, keepdims=True)
        tot1 = jnp.sum(jnp.where(even, 0.0, total), axis=1, keepdims=True)
        e = jnp.concatenate(
            [
                jnp.concatenate([jnp.where(even, x, 0.0).astype(bf16) for x in m], axis=1),
                jnp.concatenate([jnp.where(even, 0.0, x).astype(bf16) for x in m], axis=1),
            ],
            axis=0,
        )
        tops = jnp.concatenate([top0, top1], axis=0)
        tots = jnp.concatenate([tot0, tot1], axis=0)
        row0 = jnp.sum(jnp.where(diag, tops, 0.0), axis=0, keepdims=True)
        row1 = jnp.sum(jnp.where(diag, tots, 0.0), axis=0, keepdims=True)
        return e, jnp.concatenate([row0, row1], axis=0)

    def attend(bs, send=True):
        s, e = {}, {}
        for i in range(-AHEAD, len(bs) + BEHIND):
            if i + AHEAD < len(bs):
                s[i + AHEAD] = scores_of(bs[i + AHEAD])
            if 0 <= i < len(bs):
                e[i], stat[bs[i]] = softmax_of(s.pop(i))
            if i >= BEHIND:
                b = bs[i - BEHIND]
                acc[b] = jnp.dot(e.pop(i - BEHIND), vbuf[b], preferred_element_type=f32).astype(bf16)
        for b in bs if send else ():
            x_acc.copy(b).start()
            x_stat.copy(b).start()

    for i in range(1, -(-B // FLIPPED)):
        keys_wait(i)
    pltpu.make_async_copy(values, vbuf, vsem).wait()
    attend([me], send=False)
    x_near.wait_all()
    attend(near_peers)
    x_far.wait_all()
    for i in range(0, len(far_peers), UNROLL):
        attend(far_peers[i : i + UNROLL])
    gacc[me] = acc[me]
    gstat[me] = stat[me]
    for c in later:
        c.wait()
    lam = jnp.broadcast_to(lam_v[...], (heads, heads))
    lam = jnp.sum(
        jnp.where(
            lax.broadcasted_iota(jnp.int32, (heads, heads), 0)
            == lax.broadcasted_iota(jnp.int32, (heads, heads), 1),
            lam,
            0.0,
        ),
        axis=1,
        keepdims=True,
    )
    x_stat.wait_all()
    tops = [gstat[k][0:1] for k in range(n)]
    peak = tops[0]
    for t in tops[1:]:
        peak = jnp.maximum(peak, t)
    facs = [jnp.exp(t - peak) for t in tops]
    total = facs[0] * gstat[0][1:2]
    for k in range(1, n):
        total = total + facs[k] * gstat[k][1:2]
    table = jnp.transpose(
        jnp.concatenate(facs + [jnp.broadcast_to(total, (8, 128))], axis=0)
    )
    x_acc.wait_all()
    merged = table[:lines, 0:1] * gacc[0].astype(f32)
    for k in range(1, n):
        merged = merged + table[:lines, k : k + 1] * gacc[k].astype(f32)
    ratio = merged / table[:lines, n : n + 1]
    normed = []
    for g in range(kv_heads):
        base = g * 2 * half
        head = ratio[base : base + half] - lam[g * half : (g + 1) * half] * ratio[base + half : base + 2 * half]
        mean_sq = jnp.mean(head * head, axis=1, keepdims=True)
        normed.append(head * lax.rsqrt(mean_sq + 1.0 / ctx_total) * hg_v[...])
    mine_n[...] = jnp.concatenate(normed, axis=0).astype(bf16)
    x_n = ex("kv", 7, lambda p: mine_n, all_n)
    x_n.start_all()
    all_n[me] = mine_n[...]
    x_n.wait_all()

    for b in range(B):
        norm_f[b * heads : (b + 1) * heads, :] = all_n[b].astype(f32)
    normed = jnp.concatenate(
        [norm_f[pl.ds(h, B, stride=heads), :].astype(bf16) for h in range(heads)], axis=1
    )
    attn_out = jnp.dot(normed, wo_v[...], preferred_element_type=f32)
    res_v[...] = (tok_v[...].astype(f32) + attn_out).astype(bf16)
    my_y, my_c = my_tp // 2, lax.rem(my_tp, 2)
    res_sent = sent

    def res_copy(dy, dc):
        peer = lax.rem(my_y + dy, ny) * 2 + lax.rem(my_c + dc, 2)
        return remote(res_v, all_res.at[my_tp], res_sent, res_sem.at[(ny - dy) % ny], "tp", peer)

    for dy, dc in [(0, 1)] + [(d, c) for d in range(ny - 1, 0, -1) for c in range(2)]:
        res_copy(dy, dc).start()
    all_res[my_tp] = res_v[...]

    cw = up_v.shape[2]
    square = lax.broadcasted_iota(jnp.int32, (R, 128), 0) == lax.broadcasted_iota(
        jnp.int32, (R, 128), 1
    )
    chips = [lax.rem(my_y + dy, ny) for dy in range(ny)]
    ats = [rows_of(y * R, R) for y in chips]
    x_sq, x_up, x_act = [], [], []
    for dy, at in enumerate(ats):
        x_sq.append(
            Exchange(
                "kv",
                kv_peers,
                me,
                lambda p, dy=dy: sq_v.at[dy],
                lambda p, dy=dy: got_sq.at[dy, p],
                got_sq.at[dy, pl.ds(0, n - 1)],
                (sent, sems.at[11 + 3 * dy]),
            )
        )
        for xs, src_of, dst, i in (
            (x_up, lambda p, at=at: up_v.at[p, at], got_up, 12 + 3 * dy),
            (x_act, lambda p, at=at: mine_act.at[at], all_act, 13 + 3 * dy),
        ):
            xs.append(
                Exchange(
                    "kv",
                    kv_peers,
                    me,
                    src_of,
                    lambda p, dst=dst, at=at: dst.at[p, at],
                    dst.at[pl.ds(0, n - 1), at],
                    (sent, sems.at[i]),
                )
            )

    for dy, (y, at) in enumerate(zip(chips, ats)):
        arrived = all_res.at[pl.ds(0, 2 if dy else 1)]
        remote(arrived, arrived, res_sent, res_sem.at[dy], "tp", tp_peers[0]).wait_recv()
        every = all_res[pl.ds(y * 2, 2)].reshape(R, cols).astype(f32)
        gained = (every * mg_v[...]).astype(bf16)
        row_sq = jnp.sum(every * every, axis=1, keepdims=True)
        sq_v[dy] = jnp.sum(jnp.where(square, row_sq, 0.0), axis=0, keepdims=True)
        up = jnp.dot(gained, wu_v[...], preferred_element_type=f32)
        for p in range(n):
            up_v[p, at] = up[:, p * cw : (p + 1) * cw].astype(bf16)
        for peer in kv_peers:
            x_sq[dy].copy(peer).start()
            x_up[dy].copy(peer).start()
        got_sq[dy, me] = sq_v[dy]
        got_up[me, at] = up_v[me, at]
    for dy, at in enumerate(ats):
        x_sq[dy].wait_all()
        total = got_sq[dy, 0]
        for k in range(1, n):
            total = total + got_sq[dy, k]
        inv_row = lax.rsqrt(total / full_width + norm_eps)
        inv_two = jnp.sum(jnp.where(square, inv_row, 0.0), axis=1, keepdims=True)
        x_up[dy].wait_all()
        total = got_up[0, at].astype(f32)
        for k in range(1, n):
            total = total + got_up[k, at].astype(f32)
        pre = jnp.maximum(total * inv_two, 0.0)
        mine_act[at, :] = (pre * pre).astype(bf16)
        x_act[dy].start_all()
        all_act[me, at] = mine_act[at, :]

    x_down = ex("tp", 10, lambda p: down_v.at[rows_of(p * B, B)], got_down)
    for dy, (y, at) in enumerate(zip(chips, ats)):
        x_act[dy].wait_all()
        act = jnp.concatenate([all_act[k, at] for k in range(n)], axis=1)
        down_v[at, :] = jnp.dot(act, wd_v[...], preferred_element_type=f32).astype(bf16)
        for peer in [y * 2, y * 2 + 1] if dy else [y * 2 + 1 - my_c]:
            x_down.copy(peer).start()
    got_down[my_tp] = down_v[rows_of(my_tp * B, B), :]
    x_down.wait_all()
    total = got_down[0].astype(f32)
    for k in range(1, n_tp):
        total = total + got_down[k].astype(f32)
    mixed[...] = (res_v[...].astype(f32) + total).astype(bf16)

    x_kv2.wait_all()
    sent = all_res.at[pl.ds(0, n_tp - 1)]
    remote(sent, sent, res_sent, res_sem.at[0], "tp", tp_peers[0]).wait_send()
    once = [x_s, x_q, x_kv, x_far, x_near, x_kv2, x_acc, x_stat, x_n, x_down]
    for x in once + x_sq + x_up + x_act:
        x.drain()


def result_kernel(mixed, kv_out, out, new_keys, new_values, sems):
    copies = [
        pltpu.make_async_copy(src, dst, sems.at[i])
        for i, (src, dst) in enumerate(
            ((mixed, out), (kv_out.at[:, 0], new_keys), (kv_out.at[:, 1], new_values))
        )
    ]
    for c in copies:
        c.start()
    for c in copies:
        c.wait()


def shards(
    tokens,
    cache_keys,
    cache_values,
    attn_gain,
    w_query,
    w_key,
    w_value,
    lambdas,
    head_gain,
    w_out,
    mlp_gain,
    w_up,
    w_down,
):
    B, tok_width = tokens.shape
    n = lax.axis_size("kv")
    n_tp = lax.axis_size("tp")
    kv_heads = cache_keys.shape[2]
    comp = cache_keys.shape[3] // 2
    vd = cache_values.shape[3]
    ctx = cache_keys.shape[1]
    heads = lambdas.shape[0]
    span = ctx * kv_heads
    all_rows = B * n_tp
    hidden = w_up.shape[1]
    cw = hidden // n
    lines = 2 * heads
    assert B == n and comp * 2 == 128 and vd == 128
    V = pltpu.VMEM
    scratch = [
        V(tokens.shape, bf16),
        V((1, tok_width), f32),
        V(w_query.shape, bf16),
        V(w_key.shape, bf16),
        V(w_value.shape, bf16),
        V((1, heads), f32),
        V((1, vd), f32),
        V((1, tok_width), f32),
        V((B, span, 128), bf16),
        V((B, span, 128), bf16),
        V(w_out.shape, bf16),
        V(w_up.shape, bf16),
        V(w_down.shape, bf16),
        DMA((11,)),
        DMA((-(-B // FLIPPED),)),
        DMA,
        V((B * heads, 128), f32),
        V((B, 1, 128), f32),
        V((B * 8, 128), f32),
        V((n, heads, 128), f32),
        V((n, 1, 128), f32),
        V((n, 8, 128), f32),
        V((heads, 128), bf16),
        V((2, kv_heads, 128), bf16),
        V((n, heads, 128), bf16),
        V((n, lines, vd), bf16),
        V((n, 2, 128), f32),
        V((n, lines, vd), bf16),
        V((n, 2, 128), f32),
        V((heads, vd), bf16),
        V((n, heads, vd), bf16),
        V((B * heads, vd), f32),
        V((B, tok_width), bf16),
        V((n_tp, B, tok_width), bf16),
        V((n_tp // 2, 1, 128), f32),
        V((n_tp // 2, n, 1, 128), f32),
        V((n, all_rows, cw), bf16),
        V((n, all_rows, cw), bf16),
        V((all_rows, cw), bf16),
        V((n, all_rows, cw), bf16),
        V((all_rows, tok_width), bf16),
        V((n_tp, B, tok_width), bf16),
        DMA((11 + 3 * (n_tp // 2),)),
        DMA((n_tp // 2,)),
        DMA,
        V((FLIPPED, 128, span), bf16),
    ]
    mixed, kv_out = pl.pallas_call(
        functools.partial(
            layer_kernel, n, n_tp, kv_heads, tok_width * n, ctx * n, comp ** (-0.5)
        ),
        out_shape=(
            jax.ShapeDtypeStruct((B, tok_width), bf16),
            jax.ShapeDtypeStruct((n, 2, kv_heads, 128), bf16),
        ),
        in_specs=[HBM] * 13,
        out_specs=(VM, VM),
        scratch_shapes=scratch,
        compiler_params=pltpu.CompilerParams(
            collective_id=0, has_side_effects=True, vmem_limit_bytes=48 * 1024 * 1024
        ),
    )(
        *[
            pltpu.with_memory_space_constraint(x, pltpu.HBM)
            for x in (
                tokens,
                cache_keys.reshape(B, span, 128),
                cache_values.reshape(B, span, vd),
                attn_gain.reshape(1, tok_width),
                w_query,
                w_key,
                w_value,
                lambdas.reshape(1, heads),
                head_gain.reshape(1, vd),
                w_out,
                mlp_gain.reshape(1, tok_width),
                w_up,
                w_down,
            )
        ]
    )
    return pl.pallas_call(
        result_kernel,
        out_shape=(
            jax.ShapeDtypeStruct(mixed.shape, bf16),
            jax.ShapeDtypeStruct((n, kv_heads, 128), bf16),
            jax.ShapeDtypeStruct((n, kv_heads, 128), bf16),
        ),
        in_specs=[VM, VM],
        out_specs=(HBM, HBM, HBM),
        scratch_shapes=[DMA((3,))],
        compiler_params=pltpu.CompilerParams(vmem_limit_bytes=1024 * 1024),
    )(mixed, kv_out)


def solution(mesh):
    in_specs = (
        P("tp", "kv"),
        P("tp", "kv", None, None),
        P("tp", "kv", None, None),
        P("kv"),
        P("kv", None),
        P("kv", None),
        P("kv", None),
        P(),
        P(),
        P(None, "kv"),
        P("kv"),
        P("kv", "tp"),
        P("tp", "kv"),
    )
    out_specs = (P("tp", "kv"), P("tp", None, None), P("tp", None, None))
    return jax.shard_map(shards, mesh=mesh, in_specs=in_specs, out_specs=out_specs, check_vma=False)
```

```python
import functools

import jax
import jax.numpy as jnp
from jax import lax
from jax.experimental import pallas as pl
from jax.experimental.pallas import tpu as pltpu
from jax.sharding import PartitionSpec as P

norm_eps = 1e-06
f32 = jnp.float32
bf16 = jnp.bfloat16
VM = pl.BlockSpec(memory_space=pltpu.VMEM)
HBM = pl.BlockSpec(memory_space=pltpu.HBM)
DMA = pltpu.SemaphoreType.DMA
NT = (((1,), (1,)), ((), ()))
UNROLL = 6
AHEAD = 3
FLIPPED = 11
BEHIND = 2


def remote(src, dst, send, recv, axis, peer):
    return pltpu.make_async_remote_copy(
        src_ref=src,
        dst_ref=dst,
        send_sem=send,
        recv_sem=recv,
        device_id={axis: peer},
        device_id_type=pl.DeviceIdType.MESH,
    )


class Exchange:
    def __init__(self, axis, peers, me, src_of, dst_of, all_dst, sems):
        self.axis, self.peers, self.me = axis, peers, me
        self.src_of, self.dst_of, self.all_dst = src_of, dst_of, all_dst
        self.send, self.recv = sems

    def copy(self, peer):
        return remote(
            self.src_of(peer), self.dst_of(self.me), self.send, self.recv, self.axis, peer
        )

    def start_all(self):
        for peer in self.peers:
            self.copy(peer).start()

    def everything(self):
        return remote(self.all_dst, self.all_dst, self.send, self.recv, self.axis, self.peers[0])

    def wait_all(self):
        self.everything().wait_recv()

    def drain(self):
        self.everything().wait_send()


def offsets(outer, inner, wrap_inner):
    def far(d, size, wrap):
        return min(d, size - d) if wrap else d % 2

    every = [(a, b) for a in range(outer) for b in range(inner)]
    every.sort(key=lambda o: -(far(o[0], outer, True) + far(o[1], inner, wrap_inner) / 1.5))
    return every


def rows_of(start, size):
    return pl.ds(pl.multiple_of(start, size), size)


def layer_kernel(
    n,
    n_tp,
    kv_heads,
    full_width,
    ctx_total,
    scale,
    tokens,
    keys,
    values,
    attn_gain,
    w_query,
    w_key,
    w_value,
    lambdas,
    head_gain,
    w_out,
    mlp_gain,
    w_up,
    w_down,
    mixed,
    kv_out,
    tok_v,
    ag_v,
    wq_v,
    wk_v,
    wv_v,
    lam_v,
    hg_v,
    mg_v,
    kbuf,
    vbuf,
    wo_v,
    wu_v,
    wd_v,
    lsem,
    ksem,
    vsem,
    part_q,
    part_s,
    part_kv,
    got_q,
    got_s,
    got_kv,
    mine_q,
    mine_kv,
    all_q,
    acc,
    stat,
    gacc,
    gstat,
    mine_n,
    all_n,
    norm_f,
    res_v,
    all_res,
    sq_v,
    got_sq,
    up_v,
    got_up,
    mine_act,
    all_act,
    down_v,
    got_down,
    sems,
    res_sem,
    sent,
    flipped,
):
    me = lax.axis_index("kv")
    my_tp = lax.axis_index("tp")
    B = tokens.shape[0]
    heads = got_q.shape[1]
    half = heads // kv_heads
    lines = 2 * heads
    span = keys.shape[1]
    cols = tok_v.shape[1]
    all_rows = B * n_tp
    R = 2 * B
    groups = span // 128

    def order(at, outer, inner, wrap_inner):
        a, b = at // inner, lax.rem(at, inner)
        return [
            lax.rem(a + da, outer) * inner + lax.rem(b + db, inner)
            for da, db in offsets(outer, inner, wrap_inner)
        ]

    side = int(n**0.5)
    ny = n_tp // 2
    kv_order = order(me, side, side, True)
    kv_peers = kv_order[:-1]
    near_peers, far_peers = kv_order[-5:-1], kv_order[:-5]
    tp_peers = order(my_tp, ny, 2, False)[:-1]

    def ex(axis, i, src_of, dst, peers=None):
        every, at = (kv_peers, me) if axis == "kv" else (tp_peers, my_tp)
        peers = every if peers is None else peers
        return Exchange(
            axis, peers, at, src_of, lambda p: dst.at[p], dst.at[pl.ds(0, len(peers))], (sent, sems.at[i])
        )

    first = [(tokens, tok_v), (attn_gain, ag_v), (w_query, wq_v), (w_key, wk_v), (w_value, wv_v)]
    later = [
        (lambdas, lam_v),
        (head_gain, hg_v),
        (w_out, wo_v),
        (mlp_gain, mg_v),
        (w_up, wu_v),
        (w_down, wd_v),
    ]
    first = [pltpu.make_async_copy(a, b, lsem.at[i]) for i, (a, b) in enumerate(first)]
    later = [pltpu.make_async_copy(a, b, lsem.at[len(first) + i]) for i, (a, b) in enumerate(later)]
    for c in first:
        c.start()
    barrier = pltpu.get_barrier_semaphore()
    for axis, peers in (("kv", kv_peers), ("tp", tp_peers)):
        for peer in peers:
            pl.semaphore_signal(
                barrier, inc=1, device_id={axis: peer}, device_id_type=pl.DeviceIdType.MESH
            )
    for i, b in enumerate(kv_order):
        pltpu.make_async_copy(keys.at[b], kbuf.at[b], ksem.at[i // FLIPPED]).start()
    for b in kv_order:
        pltpu.make_async_copy(values.at[b], vbuf.at[b], vsem).start()

    for c in first:
        c.wait()

    def keys_wait(i):
        first, size = i * FLIPPED, min(FLIPPED, B - i * FLIPPED)
        at = pl.ds(first, size)
        pltpu.make_async_copy(keys.at[at], kbuf.at[at], ksem.at[i]).wait()

    eye = jnp.where(
        lax.broadcasted_iota(jnp.int32, (128, 128), 0)
        == lax.broadcasted_iota(jnp.int32, (128, 128), 1),
        1.0,
        0.0,
    ).astype(bf16)

    def flip():
        keys_wait(0)
        for i in range(FLIPPED):
            flipped[i] = lax.dot_general(
                eye, kbuf[kv_order[i]], NT, preferred_element_type=f32
            ).astype(bf16)

    for c in later:
        c.start()

    tok_f = tok_v[...].astype(f32)
    scaled = (tok_f * ag_v[...]).astype(bf16)
    squares = jnp.broadcast_to(jnp.sum(tok_f * tok_f, axis=1, keepdims=True), (B, 128))
    for r in range(B):
        part_s[r] = squares[r : r + 1]
    product = jnp.dot(scaled, wq_v[...], preferred_element_type=f32)
    for h in range(heads):
        part_q[pl.ds(h, B, stride=heads), :] = product[:, h * 128 : (h + 1) * 128]
    pieces = 0
    for w in (wk_v, wv_v):
        product = jnp.dot(scaled, w[...], preferred_element_type=f32)
        for h in range(product.shape[1] // 128):
            part_kv[pl.ds(pieces, B, stride=8), :] = product[:, h * 128 : (h + 1) * 128]
            pieces += 1
    for h in range(pieces, 8):
        part_kv[pl.ds(h, B, stride=8), :] = jnp.zeros((B, 128), f32)

    x_q = ex("kv", 0, lambda p: part_q.at[rows_of(p * heads, heads)], got_q)
    x_s = ex("kv", 1, lambda p: part_s.at[p], got_s)
    x_kv = ex("kv", 2, lambda p: part_kv.at[rows_of(p * 8, 8)], got_kv)
    pl.semaphore_wait(barrier, n - 1 + n_tp - 1)
    for peer in kv_peers:
        x_s.copy(peer).start()
        x_q.copy(peer).start()
    x_kv.start_all()
    got_q[me] = part_q[rows_of(me * heads, heads), :]
    got_s[me] = part_s[me]
    got_kv[me] = part_kv[rows_of(me * 8, 8), :]
    flip()
    x_s.wait_all()
    total = got_s[0]
    for k in range(1, n):
        total = total + got_s[k]
    inv_one = lax.rsqrt(total / full_width + norm_eps)
    x_q.wait_all()
    total = got_q[0]
    for k in range(1, n):
        total = total + got_q[k]
    query = (total * inv_one).astype(bf16).astype(f32) * scale
    mine_q[...] = query.astype(bf16)
    x_far = ex("kv", 3, lambda p: mine_q, all_q, far_peers)
    x_near = ex("kv", 8, lambda p: mine_q, all_q, near_peers)
    x_far.start_all()
    x_near.start_all()
    all_q[me] = mine_q[...]
    x_kv.wait_all()
    total = got_kv[0]
    for k in range(1, n):
        total = total + got_kv[k]
    new_kv = (total * inv_one).astype(bf16)
    for i in range(2):
        mine_kv[i] = new_kv[i * kv_heads : (i + 1) * kv_heads]
    x_kv2 = ex("kv", 4, lambda p: mine_kv, kv_out)
    x_kv2.start_all()
    kv_out[me] = mine_kv[...]

    lane = lax.broadcasted_iota(jnp.int32, (heads, 128), 1)
    even = lax.rem(lane, 2) == 0
    low = lane < 64
    diag = lax.broadcasted_iota(jnp.int32, (lines, 128), 1) == lax.broadcasted_iota(
        jnp.int32, (lines, 128), 0
    )

    x_acc = ex("kv", 5, lambda p: acc.at[p], gacc)
    x_stat = ex("kv", 6, lambda p: stat.at[p], gstat)

    def scores_of(b):
        q = all_q[b].astype(f32)
        lo = jnp.where(low, q, 0.0)
        hi = jnp.where(low, 0.0, q)
        q_lines = jnp.concatenate([lo[:half], hi[:half], lo[half:], hi[half:]], axis=0).astype(bf16)
        for i in range(FLIPPED):
            if b is kv_order[i]:
                return jnp.dot(q_lines, flipped[i], preferred_element_type=f32)
        return lax.dot_general(q_lines, kbuf[b], NT, preferred_element_type=f32)

    def softmax_of(s):
        m = [
            jnp.where(even, s[:heads, c * 128 : (c + 1) * 128], s[heads:, c * 128 : (c + 1) * 128])
            for c in range(groups)
        ]
        top = m[0]
        for c in range(1, groups):
            top = jnp.maximum(top, m[c])
        top0 = jnp.max(jnp.where(even, top, -jnp.inf), axis=1, keepdims=True)
        top1 = jnp.max(jnp.where(even, -jnp.inf, top), axis=1, keepdims=True)
        top = jnp.where(even, top0, top1)
        m = [jnp.exp(x - top) for x in m]
        total = m[0]
        for c in range(1, groups):
            total = total + m[c]
        tot0 = jnp.sum(jnp.where(even, total, 0.0), axis=1, keepdims=True)
        tot1 = jnp.sum(jnp.where(even, 0.0, total), axis=1, keepdims=True)
        e = jnp.concatenate(
            [
                jnp.concatenate([jnp.where(even, x, 0.0).astype(bf16) for x in m], axis=1),
                jnp.concatenate([jnp.where(even, 0.0, x).astype(bf16) for x in m], axis=1),
            ],
            axis=0,
        )
        tops = jnp.concatenate([top0, top1], axis=0)
        tots = jnp.concatenate([tot0, tot1], axis=0)
        row0 = jnp.sum(jnp.where(diag, tops, 0.0), axis=0, keepdims=True)
        row1 = jnp.sum(jnp.where(diag, tots, 0.0), axis=0, keepdims=True)
        return e, jnp.concatenate([row0, row1], axis=0)

    def attend(bs, send=True):
        s, e = {}, {}
        for i in range(-AHEAD, len(bs) + BEHIND):
            if i + AHEAD < len(bs):
                s[i + AHEAD] = scores_of(bs[i + AHEAD])
            if 0 <= i < len(bs):
                e[i], stat[bs[i]] = softmax_of(s.pop(i))
            if i >= BEHIND:
                b = bs[i - BEHIND]
                acc[b] = jnp.dot(e.pop(i - BEHIND), vbuf[b], preferred_element_type=f32).astype(bf16)
        for b in bs if send else ():
            x_acc.copy(b).start()
            x_stat.copy(b).start()

    for i in range(1, -(-B // FLIPPED)):
        keys_wait(i)
    pltpu.make_async_copy(values, vbuf, vsem).wait()
    attend([me], send=False)
    x_near.wait_all()
    attend(near_peers)
    x_far.wait_all()
    for i in range(0, len(far_peers), UNROLL):
        attend(far_peers[i : i + UNROLL])
    gacc[me] = acc[me]
    gstat[me] = stat[me]
    for c in later:
        c.wait()
    lam = jnp.broadcast_to(lam_v[...], (heads, heads))
    lam = jnp.sum(
        jnp.where(
            lax.broadcasted_iota(jnp.int32, (heads, heads), 0)
            == lax.broadcasted_iota(jnp.int32, (heads, heads), 1),
            lam,
            0.0,
        ),
        axis=1,
        keepdims=True,
    )
    x_stat.wait_all()
    tops = [gstat[k][0:1] for k in range(n)]
    peak = tops[0]
    for t in tops[1:]:
        peak = jnp.maximum(peak, t)
    facs = [jnp.exp(t - peak) for t in tops]
    total = facs[0] * gstat[0][1:2]
    for k in range(1, n):
        total = total + facs[k] * gstat[k][1:2]
    table = jnp.transpose(
        jnp.concatenate(facs + [jnp.broadcast_to(total, (8, 128))], axis=0)
    )
    x_acc.wait_all()
    merged = table[:lines, 0:1] * gacc[0].astype(f32)
    for k in range(1, n):
        merged = merged + table[:lines, k : k + 1] * gacc[k].astype(f32)
    ratio = merged / table[:lines, n : n + 1]
    normed = []
    for g in range(kv_heads):
        base = g * 2 * half
        head = ratio[base : base + half] - lam[g * half : (g + 1) * half] * ratio[base + half : base + 2 * half]
        mean_sq = jnp.mean(head * head, axis=1, keepdims=True)
        normed.append(head * lax.rsqrt(mean_sq + 1.0 / ctx_total) * hg_v[...])
    mine_n[...] = jnp.concatenate(normed, axis=0).astype(bf16)
    x_n = ex("kv", 7, lambda p: mine_n, all_n)
    x_n.start_all()
    all_n[me] = mine_n[...]
    x_n.wait_all()

    for b in range(B):
        norm_f[b * heads : (b + 1) * heads, :] = all_n[b].astype(f32)
    normed = jnp.concatenate(
        [norm_f[pl.ds(h, B, stride=heads), :].astype(bf16) for h in range(heads)], axis=1
    )
    attn_out = jnp.dot(normed, wo_v[...], preferred_element_type=f32)
    res_v[...] = (tok_v[...].astype(f32) + attn_out).astype(bf16)
    my_y, my_c = my_tp // 2, lax.rem(my_tp, 2)
    res_sent = sent

    def res_copy(dy, dc):
        peer = lax.rem(my_y + dy, ny) * 2 + lax.rem(my_c + dc, 2)
        return remote(res_v, all_res.at[my_tp], res_sent, res_sem.at[(ny - dy) % ny], "tp", peer)

    for dy, dc in [(0, 1)] + [(d, c) for d in range(ny - 1, 0, -1) for c in range(2)]:
        res_copy(dy, dc).start()
    all_res[my_tp] = res_v[...]

    cw = up_v.shape[2]
    square = lax.broadcasted_iota(jnp.int32, (R, 128), 0) == lax.broadcasted_iota(
        jnp.int32, (R, 128), 1
    )
    chips = [lax.rem(my_y + dy, ny) for dy in range(ny)]
    ats = [rows_of(y * R, R) for y in chips]
    x_sq, x_up, x_act = [], [], []
    for dy, at in enumerate(ats):
        x_sq.append(
            Exchange(
                "kv",
                kv_peers,
                me,
                lambda p, dy=dy: sq_v.at[dy],
                lambda p, dy=dy: got_sq.at[dy, p],
                got_sq.at[dy, pl.ds(0, n - 1)],
                (sent, sems.at[11 + 3 * dy]),
            )
        )
        for xs, src_of, dst, i in (
            (x_up, lambda p, at=at: up_v.at[p, at], got_up, 12 + 3 * dy),
            (x_act, lambda p, at=at: mine_act.at[at], all_act, 13 + 3 * dy),
        ):
            xs.append(
                Exchange(
                    "kv",
                    kv_peers,
                    me,
                    src_of,
                    lambda p, dst=dst, at=at: dst.at[p, at],
                    dst.at[pl.ds(0, n - 1), at],
                    (sent, sems.at[i]),
                )
            )

    for dy, (y, at) in enumerate(zip(chips, ats)):
        arrived = all_res.at[pl.ds(0, 2 if dy else 1)]
        remote(arrived, arrived, res_sent, res_sem.at[dy], "tp", tp_peers[0]).wait_recv()
        every = all_res[pl.ds(y * 2, 2)].reshape(R, cols).astype(f32)
        gained = (every * mg_v[...]).astype(bf16)
        row_sq = jnp.sum(every * every, axis=1, keepdims=True)
        sq_v[dy] = jnp.sum(jnp.where(square, row_sq, 0.0), axis=0, keepdims=True)
        up = jnp.dot(gained, wu_v[...], preferred_element_type=f32)
        for p in range(n):
            up_v[p, at] = up[:, p * cw : (p + 1) * cw].astype(bf16)
        for peer in kv_peers:
            x_sq[dy].copy(peer).start()
            x_up[dy].copy(peer).start()
        got_sq[dy, me] = sq_v[dy]
        got_up[me, at] = up_v[me, at]
    for dy, at in enumerate(ats):
        x_sq[dy].wait_all()
        total = got_sq[dy, 0]
        for k in range(1, n):
            total = total + got_sq[dy, k]
        inv_row = lax.rsqrt(total / full_width + norm_eps)
        inv_two = jnp.sum(jnp.where(square, inv_row, 0.0), axis=1, keepdims=True)
        x_up[dy].wait_all()
        total = got_up[0, at].astype(f32)
        for k in range(1, n):
            total = total + got_up[k, at].astype(f32)
        pre = jnp.maximum(total * inv_two, 0.0)
        mine_act[at, :] = (pre * pre).astype(bf16)
        x_act[dy].start_all()
        all_act[me, at] = mine_act[at, :]

    x_down = ex("tp", 10, lambda p: down_v.at[rows_of(p * B, B)], got_down)
    for dy, (y, at) in enumerate(zip(chips, ats)):
        x_act[dy].wait_all()
        act = jnp.concatenate([all_act[k, at] for k in range(n)], axis=1)
        down_v[at, :] = jnp.dot(act, wd_v[...], preferred_element_type=f32).astype(bf16)
        for peer in [y * 2, y * 2 + 1] if dy else [y * 2 + 1 - my_c]:
            x_down.copy(peer).start()
    got_down[my_tp] = down_v[rows_of(my_tp * B, B), :]
    x_down.wait_all()
    total = got_down[0].astype(f32)
    for k in range(1, n_tp):
        total = total + got_down[k].astype(f32)
    mixed[...] = (res_v[...].astype(f32) + total).astype(bf16)

    x_kv2.wait_all()
    sent = all_res.at[pl.ds(0, n_tp - 1)]
    remote(sent, sent, res_sent, res_sem.at[0], "tp", tp_peers[0]).wait_send()
    once = [x_s, x_q, x_kv, x_far, x_near, x_kv2, x_acc, x_stat, x_n, x_down]
    for x in once + x_sq + x_up + x_act:
        x.drain()


def result_kernel(mixed, kv_out, out, new_keys, new_values, sems):
    copies = [
        pltpu.make_async_copy(src, dst, sems.at[i])
        for i, (src, dst) in enumerate(
            ((mixed, out), (kv_out.at[:, 0], new_keys), (kv_out.at[:, 1], new_values))
        )
    ]
    for c in copies:
        c.start()
    for c in copies:
        c.wait()


def shards(
    tokens,
    cache_keys,
    cache_values,
    attn_gain,
    w_query,
    w_key,
    w_value,
    lambdas,
    head_gain,
    w_out,
    mlp_gain,
    w_up,
    w_down,
):
    B, tok_width = tokens.shape
    n = lax.axis_size("kv")
    n_tp = lax.axis_size("tp")
    kv_heads = cache_keys.shape[2]
    comp = cache_keys.shape[3] // 2
    vd = cache_values.shape[3]
    ctx = cache_keys.shape[1]
    heads = lambdas.shape[0]
    span = ctx * kv_heads
    all_rows = B * n_tp
    hidden = w_up.shape[1]
    cw = hidden // n
    lines = 2 * heads
    assert B == n and comp * 2 == 128 and vd == 128
    V = pltpu.VMEM
    scratch = [
        V(tokens.shape, bf16),
        V((1, tok_width), f32),
        V(w_query.shape, bf16),
        V(w_key.shape, bf16),
        V(w_value.shape, bf16),
        V((1, heads), f32),
        V((1, vd), f32),
        V((1, tok_width), f32),
        V((B, span, 128), bf16),
        V((B, span, 128), bf16),
        V(w_out.shape, bf16),
        V(w_up.shape, bf16),
        V(w_down.shape, bf16),
        DMA((11,)),
        DMA((-(-B // FLIPPED),)),
        DMA,
        V((B * heads, 128), f32),
        V((B, 1, 128), f32),
        V((B * 8, 128), f32),
        V((n, heads, 128), f32),
        V((n, 1, 128), f32),
        V((n, 8, 128), f32),
        V((heads, 128), bf16),
        V((2, kv_heads, 128), bf16),
        V((n, heads, 128), bf16),
        V((n, lines, vd), bf16),
        V((n, 2, 128), f32),
        V((n, lines, vd), bf16),
        V((n, 2, 128), f32),
        V((heads, vd), bf16),
        V((n, heads, vd), bf16),
        V((B * heads, vd), f32),
        V((B, tok_width), bf16),
        V((n_tp, B, tok_width), bf16),
        V((n_tp // 2, 1, 128), f32),
        V((n_tp // 2, n, 1, 128), f32),
        V((n, all_rows, cw), bf16),
        V((n, all_rows, cw), bf16),
        V((all_rows, cw), bf16),
        V((n, all_rows, cw), bf16),
        V((all_rows, tok_width), bf16),
        V((n_tp, B, tok_width), bf16),
        DMA((11 + 3 * (n_tp // 2),)),
        DMA((n_tp // 2,)),
        DMA,
        V((FLIPPED, 128, span), bf16),
    ]
    mixed, kv_out = pl.pallas_call(
        functools.partial(
            layer_kernel, n, n_tp, kv_heads, tok_width * n, ctx * n, comp ** (-0.5)
        ),
        out_shape=(
            jax.ShapeDtypeStruct((B, tok_width), bf16),
            jax.ShapeDtypeStruct((n, 2, kv_heads, 128), bf16),
        ),
        in_specs=[HBM] * 13,
        out_specs=(VM, VM),
        scratch_shapes=scratch,
        compiler_params=pltpu.CompilerParams(
            collective_id=0, has_side_effects=True, vmem_limit_bytes=48 * 1024 * 1024
        ),
    )(
        *[
            pltpu.with_memory_space_constraint(x, pltpu.HBM)
            for x in (
                tokens,
                cache_keys.reshape(B, span, 128),
                cache_values.reshape(B, span, vd),
                attn_gain.reshape(1, tok_width),
                w_query,
                w_key,
                w_value,
                lambdas.reshape(1, heads),
                head_gain.reshape(1, vd),
                w_out,
                mlp_gain.reshape(1, tok_width),
                w_up,
                w_down,
            )
        ]
    )
    return pl.pallas_call(
        result_kernel,
        out_shape=(
            jax.ShapeDtypeStruct(mixed.shape, bf16),
            jax.ShapeDtypeStruct((n, kv_heads, 128), bf16),
            jax.ShapeDtypeStruct((n, kv_heads, 128), bf16),
        ),
        in_specs=[VM, VM],
        out_specs=(HBM, HBM, HBM),
        scratch_shapes=[DMA((3,))],
        compiler_params=pltpu.CompilerParams(vmem_limit_bytes=1024 * 1024),
    )(mixed, kv_out)


def solution(mesh):
    in_specs = (
        P("tp", "kv"),
        P("tp", "kv", None, None),
        P("tp", "kv", None, None),
        P("kv"),
        P("kv", None),
        P("kv", None),
        P("kv", None),
        P(),
        P(),
        P(None, "kv"),
        P("kv"),
        P("kv", "tp"),
        P("tp", "kv"),
    )
    out_specs = (P("tp", "kv"), P("tp", None, None), P("tp", None, None))
    return jax.shard_map(shards, mesh=mesh, in_specs=in_specs, out_specs=out_specs, check_vma=False)
```
